128 devices in a mesh: ep: 64 (over z, y, x), tp: 2 (over core).
Axes of the slice: x: 4, y: 4, z: 4, core: 2. Of those that a mesh axis runs over, the one named last changes fastest.
Arguments:
- hidden: bfloat16 [4096, 2048], P('ep'), may hold values from -6 to 6
- mix_gain: float32 [2048], replicated, may hold values from 0.1 to 1.9
- recept_weight: bfloat16 [2048, 1024], P(None, 'tp'), may hold values from -0.125 to 0.125
- key_weight: bfloat16 [2048, 1024], P(None, 'tp'), may hold values from -0.125 to 0.125
- value_weight: bfloat16 [2048, 1024], P(None, 'tp'), may hold values from -0.125 to 0.125
- decay_down: bfloat16 [2048, 64], replicated, may hold values from -0.125 to 0.125
- decay_up: bfloat16 [64, 1024], replicated, may hold values from -0.75 to 0.75
- decay_bias: float32 [1024], replicated, may hold values from -4 to 1
- rate_down: bfloat16 [2048, 64], replicated, may hold values from -0.125 to 0.125
- rate_up: bfloat16 [64, 1024], replicated, may hold values from -0.75 to 0.75
- rate_bias: float32 [1024], replicated, may hold values from -4 to 4
- head_gain: float32 [1024], replicated, may hold values from 0.1 to 1.9
- out_weight: bfloat16 [1024, 2048], P('tp'), may hold values from -0.1875 to 0.1875
- memory_state: float32 [4096, 16, 64, 64], P('ep', 'tp'), may hold values from -6 to 6
- ffn_gain: float32 [2048], replicated, may hold values from 0.1 to 1.9
- blend_vector: bfloat16 [2048], replicated, may hold values from -0.125 to 0.125
- dense_gate: bfloat16 [2048, 5632], P(None, ('ep', 'tp')), may hold values from -0.125 to 0.125
- dense_up: bfloat16 [2048, 5632], P(None, ('ep', 'tp')), may hold values from -0.125 to 0.125
- dense_down: bfloat16 [5632, 2048], P(('ep', 'tp')), may hold values from -0.3125 to 0.3125
- expert_gate: bfloat16 [64, 2048, 1536], P('ep', None, 'tp'), may hold values from -0.125 to 0.125
- expert_up: bfloat16 [64, 2048, 1536], P('ep', None, 'tp'), may hold values from -0.125 to 0.125
- expert_down: bfloat16 [64, 1536, 2048], P('ep', 'tp'), may hold values from -0.15625 to 0.15625
- routing: int32 [4096, 2], P('ep'), may hold values from 0 to 63, all different within a row; in each aligned block of 64 rows (0 to 63, 64 to 127, ...) at most 4 rows name the same one
- route_scale: float32 [4096, 2], P('ep'), may hold values from 0.25 to 1
Outputs:
- layer_out: bfloat16 [4096, 2048], P('ep')
- new_state: float32 [4096, 16, 64, 64], P('ep', 'tp')
The draws below stay inside these ranges and needn't reach their ends.
Inputs may be any that keep to these rules, and one draw needn't show every extreme that they name: `routing`: among the 64 sequences of one index of ep, no expert is chosen more than 4 times, and some expert is chosen exactly 4 times; a sequence's 2 choices differ.
All inputs are finite; a program needn't handle non-finite values.
Results may differ from the reference program's by a relative error of at most 0.017.
Values may be sent and summed in bfloat16 or wider, within the bound.
A program may use at most 192 MiB of HBM per device.

```python
import math
import jax
import jax.numpy as jnp
import numpy as np
from jax import lax

D = 2048
HEADS = 16
HEAD = 64
LOW = 64
DFF = 5632
EFF = 1536
TOPK = 2
SEQS = 64
SEQUENCES = 4096
EXPERTS = 64
CAP = 4
N_EP = 64
N_TP = 2


def block_scale(stream_key, dims, pieces, least, largest):
    def one(position, blocks):
        steps = jax.random.uniform(jax.random.fold_in(jax.random.fold_in(stream_key, 6), position), (blocks,), jnp.float32, least / len(pieces), largest / len(pieces))
        return jnp.repeat(jnp.exp(steps), dims[position] // blocks).reshape((-1,) + (1,) * (len(dims) - position - 1))

    factor_of = one(*pieces[0])
    for cut in pieces[1:]:
        factor_of = factor_of * one(*cut)
    return factor_of


def assign_block(own_key, own, number, rows, number_of, top, most, lean):
    ranking = jax.random.permutation(own_key, number_of)
    packed, common = portions_of(number_of, rows * top, most, lean, True), portions_of(number_of, rows * top, most, lean, False)
    places = jnp.arange(number_of)

    def named(sizes, offset_by):
        used = int((sizes > 0).sum())
        fixed = max(1, used // 4)
        passed = fixed + (places - fixed + offset_by * (used - fixed)) % max(1, number_of - fixed)
        return jnp.zeros((number_of,), jnp.int32).at[ranking[jnp.where(places < fixed, places, passed)]].set(jnp.asarray(sizes, jnp.int32))

    sizes = jnp.where(number % 4 == 0, named(packed, number // 4), named(common, number - number // 4 - 1))
    mixed = jax.random.permutation(jax.random.fold_in(own, 3), number_of)
    donor, receiver = mixed[0:number_of // 2 * 2:2], mixed[1:number_of // 2 * 2:2]
    slack = jnp.minimum(sizes[donor] - 1, most - sizes[receiver]) // 2
    slack = jnp.where((donor == ranking[0]) | (receiver == ranking[0]) | (sizes[receiver] == 0), 0, jnp.maximum(slack, 0))
    passed = jax.random.randint(jax.random.fold_in(own, 4), (number_of // 2,), 0, 1 << 20) % (slack + 1)
    sizes = sizes.at[donor].add(-passed).at[receiver].add(passed)
    members = jnp.searchsorted(jnp.cumsum(sizes), jnp.arange(rows * top), side="right").astype(jnp.int32)
    listing = members.reshape(top, rows).T
    listing = listing[jax.random.permutation(jax.random.fold_in(own, 1), rows)]
    offset_by = jax.random.randint(jax.random.fold_in(own, 2), (rows, 1), 0, top)
    return jnp.take_along_axis(listing, (jnp.arange(top)[None, :] + offset_by) % top, axis=1)


def portions_of(count, total, most, lean, full):
    portions = [(1 << 20) // math.isqrt(grade ** lean) + 1 for grade in range(1, count + 1)]
    largest = most if full else min(most, max(-(-total // count), total * portions[0] // sum(portions)))
    least = 1 if total - largest >= count - 1 else 0
    counts, rest = [largest] + [least] * (count - 1), total - largest - least * (count - 1)
    while rest > 0:
        movable = [i for i in range(1, count) if counts[i] < largest] or [i for i in range(1, count) if counts[i] < most]
        pool, remaining = sum([portions[i] for i in movable]), rest
        for i in movable:
            extra = min(most - counts[i], max(1, remaining * portions[i] // pool), rest)
            counts[i] = counts[i] + extra
            rest = rest - extra
    return np.array(counts)


def scatter_about(key, shape, width, bound, pieces=(), held_as=jnp.bfloat16):
    values = jax.random.normal(key, shape, jnp.float32) * width
    if len(pieces) > 0:
        values = block_scale(key, shape, pieces, -0.22, 0.18) * values
    return jnp.clip(values, min=-bound, max=bound).astype(held_as)


def setup_inputs(seed: int = 0) -> dict:
    arg_keys = jax.random.split(jax.random.key(seed), 25)
    hidden = scatter_about(arg_keys[0], (SEQUENCES, D), 1.0, 6.0, ((0, 64),))
    mix_gain = jnp.clip(1.0 + 0.18 * jax.random.normal(arg_keys[1], (D,), jnp.float32), 0.1, 1.9)
    recept_weight = scatter_about(arg_keys[2], (D, HEADS * HEAD), D ** -0.5, 0.125, ((1, 2),))
    key_weight = scatter_about(arg_keys[3], (D, HEADS * HEAD), D ** -0.5, 0.125, ((1, 2),))
    value_weight = scatter_about(arg_keys[4], (D, HEADS * HEAD), D ** -0.5, 0.125, ((1, 2),))
    decay_down = scatter_about(arg_keys[5], (D, LOW), D ** -0.5, 0.125)
    decay_up = scatter_about(arg_keys[6], (LOW, HEADS * HEAD), LOW ** -0.5, 0.75)
    decay_bias = jnp.clip(jax.random.uniform(arg_keys[7], (HEADS * HEAD,), jnp.float32, -4.0, 1.0), -4.0, 1.0)
    rate_down = scatter_about(arg_keys[8], (D, LOW), D ** -0.5, 0.125)
    rate_up = scatter_about(arg_keys[9], (LOW, HEADS * HEAD), LOW ** -0.5, 0.75)
    rate_bias = scatter_about(arg_keys[10], (HEADS * HEAD,), 1.0, 4.0, (), jnp.float32)
    head_gain = jnp.clip(1.0 + 0.18 * jax.random.normal(arg_keys[11], (HEADS * HEAD,), jnp.float32), 0.1, 1.9)
    out_weight = scatter_about(arg_keys[12], (HEADS * HEAD, D), (HEADS * HEAD) ** -0.5, 0.1875, ((0, 2),))
    memory_state = scatter_about(arg_keys[13], (SEQUENCES, HEADS, HEAD, HEAD), 1.0, 6.0, ((0, 64), (1, 2)), jnp.float32)
    ffn_gain = jnp.clip(1.0 + 0.18 * jax.random.normal(arg_keys[14], (D,), jnp.float32), 0.1, 1.9)
    blend_vector = scatter_about(arg_keys[15], (D,), D ** -0.5, 0.125)
    dense_gate = scatter_about(arg_keys[16], (D, DFF), D ** -0.5, 0.125, ((1, 128),))
    dense_up = scatter_about(arg_keys[17], (D, DFF), D ** -0.5, 0.125, ((1, 128),))
    dense_down = scatter_about(arg_keys[18], (DFF, D), (DFF // 16) ** -0.5, 0.3125, ((0, 128),))
    expert_gate = scatter_about(arg_keys[19], (EXPERTS, D, EFF), D ** -0.5, 0.125, ((0, 64), (2, 2)))
    expert_up = scatter_about(arg_keys[20], (EXPERTS, D, EFF), D ** -0.5, 0.125, ((0, 64), (2, 2)))
    expert_down = scatter_about(arg_keys[21], (EXPERTS, EFF, D), EFF ** -0.5, 0.15625, ((0, 64), (1, 2)))
    routing_keys = jax.random.split(jax.random.fold_in(arg_keys[22], 1), SEQUENCES // SEQS)
    routing_turns = jax.random.permutation(jax.random.fold_in(arg_keys[22], 3), SEQUENCES // SEQS)
    routing = jax.vmap(lambda own, number: assign_block(jax.random.fold_in(arg_keys[22], 2), own, number, SEQS, EXPERTS, TOPK, CAP, 1))(routing_keys, routing_turns).reshape((SEQUENCES, TOPK))
    route_scale = jnp.clip(0.25 + 0.75 * jax.random.uniform(arg_keys[23], (SEQUENCES, TOPK), jnp.float32) ** block_scale(arg_keys[23], (SEQUENCES, TOPK), ((0, 64),), -0.2, 0.2), 0.25, 1.0)
    return {"hidden": hidden, "mix_gain": mix_gain, "recept_weight": recept_weight, "key_weight": key_weight, "value_weight": value_weight, "decay_down": decay_down, "decay_up": decay_up, "decay_bias": decay_bias, "rate_down": rate_down, "rate_up": rate_up, "rate_bias": rate_bias, "head_gain": head_gain, "out_weight": out_weight, "memory_state": memory_state, "ffn_gain": ffn_gain, "blend_vector": blend_vector, "dense_gate": dense_gate, "dense_up": dense_up, "dense_down": dense_down, "expert_gate": expert_gate, "expert_up": expert_up, "expert_down": expert_down, "routing": routing, "route_scale": route_scale}


def stored(tensor):
    return lax.optimization_barrier(tensor.astype(jnp.bfloat16)).astype(jnp.float32)

def rms_scaled(tensor, gain_vec):
    values = tensor.astype(jnp.float32)
    return values * lax.rsqrt(lax.optimization_barrier(jnp.mean(values * values, axis=-1, keepdims=True)) + 1e-06) * gain_vec

def silu_of(tensor):
    return tensor / (1.0 + jnp.exp(-tensor))

def matmul(left, right):
    return jnp.dot(left, right, preferred_element_type=jnp.float32)

def reference(hidden, mix_gain, recept_weight, key_weight, value_weight, decay_down, decay_up, decay_bias, rate_down, rate_up, rate_bias, head_gain, out_weight, memory_state, ffn_gain, blend_vector, dense_gate, dense_up, dense_down, expert_gate, expert_up, expert_down, routing, route_scale):
    seq_count = hidden.shape[0]
    full_width = HEADS * HEAD
    normed_in = rms_scaled(hidden, mix_gain).astype(jnp.bfloat16)
    recept_rows = stored(matmul(normed_in, recept_weight)).reshape(seq_count, HEADS, HEAD)
    key_rows = stored(matmul(normed_in, key_weight)).reshape(seq_count, HEADS, HEAD)
    value_rows = stored(matmul(normed_in, value_weight)).reshape(seq_count, HEADS, HEAD)
    decay_low = jnp.tanh(matmul(normed_in, decay_down)).astype(jnp.bfloat16)
    decay_pre = matmul(decay_low, decay_up) + decay_bias
    decay_rate = jnp.exp(-jnp.exp(-jax.nn.softplus(-decay_pre) - 0.5)).reshape(seq_count, HEADS, HEAD)
    rate_low = matmul(normed_in, rate_down).astype(jnp.bfloat16)
    learn_rate = jax.nn.sigmoid(matmul(rate_low, rate_up) + rate_bias).reshape(seq_count, HEADS, HEAD)
    unit_key = key_rows * lax.rsqrt(lax.optimization_barrier(jnp.sum(key_rows * key_rows, axis=-1, keepdims=True)) + 1e-06)
    removed = jnp.einsum('shij,shj->shi', memory_state, unit_key, precision=lax.Precision.HIGHEST)
    new_state = memory_state * decay_rate[:, :, None, :] - removed[..., None] * (unit_key * learn_rate)[:, :, None, :] + value_rows[..., None] * (key_rows * learn_rate)[:, :, None, :]
    readout = jnp.einsum('shij,shj->shi', new_state, recept_rows, precision=lax.Precision.HIGHEST)
    centre = lax.optimization_barrier(jnp.mean(readout, axis=-1, keepdims=True))
    variance = lax.optimization_barrier(jnp.mean(jnp.square(readout - centre), axis=-1, keepdims=True))
    head_normed = ((readout - centre) * lax.rsqrt(variance + 0.00064) * head_gain.reshape(HEADS, HEAD)).astype(jnp.bfloat16).reshape(seq_count, full_width)
    group_width = full_width // N_TP
    attn_sum = jnp.zeros((seq_count, D), jnp.float32)
    for group in range(N_TP):
        lower = group * group_width
        attn_sum = attn_sum + stored(matmul(head_normed[:, lower:lower + group_width], out_weight[lower:lower + group_width]))
    first_res = (hidden.astype(jnp.float32) + attn_sum).astype(jnp.bfloat16)
    ffn_in = rms_scaled(first_res, ffn_gain).astype(jnp.bfloat16)
    blend = jax.nn.sigmoid(jnp.dot(ffn_in, blend_vector, preferred_element_type=jnp.float32))
    dense_act = (silu_of(matmul(ffn_in, dense_gate)) * matmul(ffn_in, dense_up)).astype(jnp.bfloat16)
    dense_out = matmul(dense_act, dense_down)
    flat_route = routing.reshape(-1)
    flat_scale = route_scale.reshape(-1)
    slot_total = N_EP * CAP
    slot_index = jnp.arange(slot_total, dtype=jnp.int32)

    def one_expert(total, inputs):
        gate_mat, up_mat, down_mat, index = inputs
        chosen = flat_route == index
        live_count = jnp.sum(chosen.astype(jnp.int32))
        picks = jnp.nonzero(chosen, size=slot_total, fill_value=0)[0].astype(jnp.int32)
        owners = (picks // TOPK).astype(jnp.int32)
        rows = ffn_in[owners]
        live = slot_index < live_count
        scales = jnp.where(live, flat_scale[picks], jnp.zeros_like(flat_scale[picks]))
        expert_act = (silu_of(matmul(rows, gate_mat)) * matmul(rows, up_mat)).astype(jnp.bfloat16)
        expert_out = matmul(expert_act, down_mat)
        return (total.at[owners].add(expert_out * scales[:, None]), None)
    expert_sum, _ = lax.scan(one_expert, jnp.zeros((seq_count, D), jnp.float32), (expert_gate, expert_up, expert_down, jnp.arange(EXPERTS, dtype=jnp.int32)))
    layer_out = (first_res.astype(jnp.float32) + expert_sum + blend[:, None] * dense_out).astype(jnp.bfloat16)
    return (layer_out, new_state)
```

```python
import jax
import jax.numpy as jnp
from jax import lax
from jax.experimental import pallas as pl
from jax.experimental.pallas import tpu as pltpu
from jax.sharding import PartitionSpec as P

SB = 8


def att_kernel(
    hid_ref, mixg_ref, wr_ref, wk_ref, wv_ref, dd_ref, du_ref, db_ref, rd_ref, ru_ref, rb_ref, hg_ref, ow_ref,
    st_ref, ns_ref, gp_ref, k_s, d_s, l_s, q_s, v_s, b_s, yt_s,
):
    step = pl.program_id(0)
    heads, size = 8, 64
    width = heads * size

    @pl.when(step == 0)
    def _():
        own = pl.ds(pl.multiple_of(lax.axis_index("tp") * width, width), width)
        x = hid_ref[...].astype(jnp.float32)
        scale = lax.rsqrt(jnp.mean(x * x, axis=-1, keepdims=True) + 1e-06)
        nb = (x * scale * mixg_ref[...]).astype(jnp.bfloat16)
        low = jnp.tanh(nt_dot(nb, dd_ref[...])).astype(jnp.bfloat16)
        pre = dot(low, du_ref[:, own]) + db_ref[:, own]
        dec = jnp.exp(-jnp.exp(-0.5) * (1.0 / (1.0 + jnp.exp(-pre))))
        rlow = nt_dot(nb, rd_ref[...]).astype(jnp.bfloat16)
        lr = 1.0 / (1.0 + jnp.exp(-(dot(rlow, ru_ref[:, own]) + rb_ref[:, own])))
        key = dot(nb, wk_ref[...]).astype(jnp.bfloat16).astype(jnp.float32)
        val = dot(nb, wv_ref[...]).astype(jnp.bfloat16).astype(jnp.float32)
        rec = dot(nb, wr_ref[...]).astype(jnp.bfloat16).astype(jnp.float32)
        for h in range(heads):
            cut = slice(h * size, (h + 1) * size)
            kh, dh, lh, rh = key[:, cut], dec[:, cut], lr[:, cut], rec[:, cut]
            rn2 = 1.0 / (jnp.sum(kh * kh, axis=-1, keepdims=True) + 1e-06)
            kl = kh * lh
            k_s[h] = kh * rn2
            d_s[h] = dh
            l_s[h] = kl
            q_s[h] = dh * rh
            v_s[h] = val[:, cut]
            b_s[h] = jnp.broadcast_to(jnp.sum(kl * rh, axis=-1, keepdims=True), (64, size))

    eye = (
        lax.broadcasted_iota(jnp.int32, (size, size), 0) == lax.broadcasted_iota(jnp.int32, (size, size), 1)
    )
    lane = lax.broadcasted_iota(jnp.int32, (size, 128), 1)

    def one(j, _):
        for u in range(2):
            sl = j * 2 + u
            s = step * SB + sl
            row = pl.ds(s, 1)
            for h in range(heads):
                m = st_ref[sl, h]
                t = jnp.where(eye, v_s[h, row, :], 0.0) - m * k_s[h, row, :]
                w = jnp.sum(t, axis=-1, keepdims=True)
                y0 = jnp.sum(m * q_s[h, row, :], axis=-1, keepdims=True)
                ns_ref[sl, h] = m * d_s[h, row, :] + w * l_s[h, row, :]
                y = y0 + w * b_s[h, row, 0:1]
                yt_s[h] = jnp.where(lane == s, y, yt_s[h])
        return 0

    lax.fori_loop(0, SB // 2, one, 0)

    @pl.when(step == pl.num_programs(0) - 1)
    def _():
        parts = []
        for h in range(heads):
            y = yt_s[h]
            c = y - jnp.mean(y, axis=0, keepdims=True)
            var = jnp.mean(c * c, axis=0, keepdims=True)
            parts.append(c * lax.rsqrt(var + 0.00064))
        full = jnp.concatenate(parts, axis=0).T[:64]
        hn = (full * hg_ref[:, pl.ds(pl.multiple_of(lax.axis_index("tp") * width, width), width)]).astype(jnp.bfloat16)
        gp_ref[...] = dot(hn, ow_ref[...]).astype(jnp.bfloat16)


def dot(a, b):
    return jnp.dot(a, b, preferred_element_type=jnp.float32)


def nt_dot(a, b):
    return lax.dot_general(a, b, (((1,), (1,)), ((), ())), preferred_element_type=jnp.float32)


def attention(hidden, mix_gain, wr, wk, wv, dd, du, db, rd, ru, rb, hg, ow, state):
    seqs = hidden.shape[0]
    whole = lambda shape: pl.BlockSpec(shape, lambda g: tuple(0 for _ in shape))
    ops = [
        hidden, mix_gain.reshape(1, -1), wr, wk, wv, dd.T, du, db.reshape(1, -1), rd.T, ru, rb.reshape(1, -1),
        hg.reshape(1, -1), ow,
    ]
    blk = pl.BlockSpec((SB, 8, 64, 64), lambda g: (g, 0, 0, 0))
    small = pltpu.VMEM((8, seqs, 64), jnp.float32)
    new_state, part = pl.pallas_call(
        att_kernel,
        grid=(seqs // SB,),
        in_specs=[whole(o.shape) for o in ops] + [blk],
        out_specs=[blk, whole((seqs, 2048))],
        out_shape=[
            jax.ShapeDtypeStruct(state.shape, jnp.float32),
            jax.ShapeDtypeStruct((seqs, 2048), jnp.bfloat16),
        ],
        scratch_shapes=[small] * 6 + [pltpu.VMEM((8, 64, 128), jnp.float32)],
        compiler_params=pltpu.CompilerParams(
            dimension_semantics=("arbitrary",), vmem_limit_bytes=60 * 1024 * 1024
        ),
        cost_estimate=pl.CostEstimate(flops=40_000_000_000, bytes_accessed=44_000_000, transcendentals=0),
        name="attention",
    )(*ops, state)
    return new_state, part


def copy_for_each(x, axis):
    length = lax.axis_size(axis)
    return lax.all_to_all(jnp.broadcast_to(x[None], (length, *x.shape)), axis, 0, 0, tiled=True)


def of_everyone(x, axis):
    everything = copy_for_each(x, axis)
    return jnp.sum(everything.astype(jnp.float32), axis=0)


def stored(tensor):
    return lax.optimization_barrier(tensor.astype(jnp.bfloat16)).astype(jnp.float32)


def rms_scaled(tensor, gain_vec):
    values = tensor.astype(jnp.float32)
    return values * lax.rsqrt(jnp.mean(values * values, axis=-1, keepdims=True) + 1e-06) * gain_vec


def silu_of(tensor):
    return tensor / (1.0 + jnp.exp(-tensor))


def matmul(left, right):
    return jnp.dot(left, right, preferred_element_type=jnp.float32)


def shards(
    hidden,
    mix_gain,
    recept_weight,
    key_weight,
    value_weight,
    decay_down,
    decay_up,
    decay_bias,
    rate_down,
    rate_up,
    rate_bias,
    head_gain,
    out_weight,
    memory_state,
    ffn_gain,
    blend_vector,
    dense_gate,
    dense_up,
    dense_down,
    expert_gate,
    expert_up,
    expert_down,
    routing,
    route_scale,
):
    seq_count, model_width = hidden.shape
    new_state, part = attention(
        hidden, mix_gain, recept_weight, key_weight, value_weight, decay_down, decay_up, decay_bias,
        rate_down, rate_up, rate_bias, head_gain, out_weight, memory_state,
    )
    attn_sum = of_everyone(part, "tp").astype(
        jnp.float32
    )
    first_res = (hidden.astype(jnp.float32) + attn_sum).astype(jnp.bfloat16)
    ffn_in = rms_scaled(first_res, ffn_gain).astype(jnp.bfloat16)
    blend = jax.nn.sigmoid(jnp.dot(ffn_in, blend_vector, preferred_element_type=jnp.float32))
    piece = lax.all_gather(ffn_in, "ep", axis=0, tiled=True)
    dense_act = (silu_of(matmul(piece, dense_gate)) * matmul(piece, dense_up)).astype(jnp.bfloat16)
    own_units = lax.all_to_all(dense_act, "ep", split_axis=0, concat_axis=1, tiled=True)
    dense_out = matmul(own_units, lax.all_gather(dense_down, "ep", axis=0, tiled=True))
    dest_count = lax.axis_size("ep")
    top_count = routing.shape[1]
    slot_cap = max(2, 2 * seq_count * top_count // dest_count)
    flat_route = routing.reshape(-1)
    one_hot = (flat_route[:, None] == jnp.arange(dest_count, dtype=jnp.int32)[None, :]).astype(
        jnp.int32
    )
    running = jnp.cumsum(one_hot, axis=0)
    rank = jnp.sum((running - 1) * one_hot, axis=1)
    slot = flat_route * slot_cap + rank
    select = (slot[None, :] == jnp.arange(dest_count * slot_cap, dtype=jnp.int32)[:, None]).astype(
        jnp.bfloat16
    )
    pair_rows = jnp.repeat(ffn_in, top_count, axis=0)
    outgoing = (
        matmul(select, pair_rows).astype(jnp.bfloat16).reshape(dest_count, slot_cap, model_width)
    )
    arrived = lax.all_to_all(outgoing, "ep", split_axis=0, concat_axis=0, tiled=True)
    src_count, slot_items, width_in = arrived.shape
    flat_in = arrived.reshape(src_count * slot_items, width_in)
    expert_act = (silu_of(matmul(flat_in, expert_gate[0])) * matmul(flat_in, expert_up[0])).astype(
        jnp.bfloat16
    )
    result = matmul(expert_act, expert_down[0]).reshape(src_count, slot_items, width_in)
    returned = lax.all_to_all(
        result.astype(jnp.bfloat16), "ep", split_axis=0, concat_axis=0, tiled=True
    ).astype(result.dtype)
    per_pair = jnp.take(returned.reshape(dest_count * slot_cap, model_width), slot, axis=0)
    expert_sum = jnp.sum(
        per_pair.reshape(seq_count, top_count, model_width) * route_scale[:, :, None], axis=1
    )
    mixed = of_everyone(
        (expert_sum + blend[:, None] * dense_out).astype(jnp.bfloat16), "tp"
    ).astype(jnp.float32)
    layer_out = (first_res.astype(jnp.float32) + mixed).astype(jnp.bfloat16)
    return (layer_out, new_state)


def solution(mesh):
    in_specs = (
        P("ep", None),
        P(),
        P(None, "tp"),
        P(None, "tp"),
        P(None, "tp"),
        P(),
        P(),
        P(),
        P(),
        P(),
        P(),
        P(),
        P("tp", None),
        P("ep", "tp", None, None),
        P(),
        P(),
        P(None, ("ep", "tp")),
        P(None, ("ep", "tp")),
        P(("ep", "tp"), None),
        P("ep", None, "tp"),
        P("ep", None, "tp"),
        P("ep", "tp", None),
        P("ep", None),
        P("ep", None),
    )
    out_specs = (P("ep", None), P("ep", "tp", None, None))
    return jax.shard_map(shards, mesh=mesh, in_specs=in_specs, out_specs=out_specs, check_vma=False)
```

```python
import jax
import jax.numpy as jnp
from jax import lax
from jax.experimental import pallas as pl
from jax.experimental.pallas import tpu as pltpu
from jax.sharding import PartitionSpec as P

MESH = pl.DeviceIdType.MESH
SB = 8


def att_kernel(
    hid_ref, mixg_ref, wr_ref, wk_ref, wv_ref, dd_ref, du_ref, db_ref, rd_ref, ru_ref, rb_ref, hg_ref, ow_ref,
    st_ref, ns_ref, gp_ref, k_s, d_s, l_s, q_s, v_s, b_s, yt_s,
):
    step = pl.program_id(0)
    heads, size = 8, 64
    width = heads * size

    @pl.when(step == 0)
    def _():
        own = pl.ds(pl.multiple_of(lax.axis_index("tp") * width, width), width)
        x = hid_ref[...].astype(jnp.float32)
        scale = lax.rsqrt(jnp.mean(x * x, axis=-1, keepdims=True) + 1e-06)
        nb = (x * scale * mixg_ref[...]).astype(jnp.bfloat16)
        low = jnp.tanh(nt_dot(nb, dd_ref[...])).astype(jnp.bfloat16)
        pre = dot(low, du_ref[:, own]) + db_ref[:, own]
        dec = jnp.exp(-jnp.exp(-0.5) * (1.0 / (1.0 + jnp.exp(-pre))))
        rlow = nt_dot(nb, rd_ref[...]).astype(jnp.bfloat16)
        lr = 1.0 / (1.0 + jnp.exp(-(dot(rlow, ru_ref[:, own]) + rb_ref[:, own])))
        key = dot(nb, wk_ref[...]).astype(jnp.bfloat16).astype(jnp.float32)
        val = dot(nb, wv_ref[...]).astype(jnp.bfloat16).astype(jnp.float32)
        rec = dot(nb, wr_ref[...]).astype(jnp.bfloat16).astype(jnp.float32)
        for h in range(heads):
            cut = slice(h * size, (h + 1) * size)
            kh, dh, lh, rh = key[:, cut], dec[:, cut], lr[:, cut], rec[:, cut]
            rn2 = 1.0 / (jnp.sum(kh * kh, axis=-1, keepdims=True) + 1e-06)
            kl = kh * lh
            k_s[h] = kh * rn2
            d_s[h] = dh
            l_s[h] = kl
            q_s[h] = dh * rh
            v_s[h] = val[:, cut]
            b_s[h] = jnp.broadcast_to(jnp.sum(kl * rh, axis=-1, keepdims=True), (64, size))

    eye = (
        lax.broadcasted_iota(jnp.int32, (size, size), 0) == lax.broadcasted_iota(jnp.int32, (size, size), 1)
    )
    lane = lax.broadcasted_iota(jnp.int32, (size, 128), 1)

    def one(j, _):
        for u in range(2):
            sl = j * 2 + u
            s = step * SB + sl
            row = pl.ds(s, 1)
            for h in range(heads):
                m = st_ref[sl, h]
                t = jnp.where(eye, v_s[h, row, :], 0.0) - m * k_s[h, row, :]
                w = jnp.sum(t, axis=-1, keepdims=True)
                y0 = jnp.sum(m * q_s[h, row, :], axis=-1, keepdims=True)
                ns_ref[sl, h] = m * d_s[h, row, :] + w * l_s[h, row, :]
                y = y0 + w * b_s[h, row, 0:1]
                yt_s[h] = jnp.where(lane == s, y, yt_s[h])
        return 0

    lax.fori_loop(0, SB // 2, one, 0)

    @pl.when(step == pl.num_programs(0) - 1)
    def _():
        parts = []
        for h in range(heads):
            y = yt_s[h]
            c = y - jnp.mean(y, axis=0, keepdims=True)
            var = jnp.mean(c * c, axis=0, keepdims=True)
            parts.append(c * lax.rsqrt(var + 0.00064))
        full = jnp.concatenate(parts, axis=0).T[:64]
        hn = (full * hg_ref[:, pl.ds(pl.multiple_of(lax.axis_index("tp") * width, width), width)]).astype(jnp.bfloat16)
        gp_ref[...] = dot(hn, ow_ref[...]).astype(jnp.bfloat16)


def dot(a, b):
    return jnp.dot(a, b, preferred_element_type=jnp.float32)


def nt_dot(a, b):
    return lax.dot_general(a, b, (((1,), (1,)), ((), ())), preferred_element_type=jnp.float32)


def attention(hidden, mix_gain, wr, wk, wv, dd, du, db, rd, ru, rb, hg, ow, state):
    seqs = hidden.shape[0]
    whole = lambda shape: pl.BlockSpec(shape, lambda g: tuple(0 for _ in shape))
    ops = [
        hidden, mix_gain.reshape(1, -1), wr, wk, wv, dd.T, du, db.reshape(1, -1), rd.T, ru, rb.reshape(1, -1),
        hg.reshape(1, -1), ow,
    ]
    blk = pl.BlockSpec((SB, 8, 64, 64), lambda g: (g, 0, 0, 0))
    small = pltpu.VMEM((8, seqs, 64), jnp.float32)
    new_state, part = pl.pallas_call(
        att_kernel,
        grid=(seqs // SB,),
        in_specs=[whole(o.shape) for o in ops] + [blk],
        out_specs=[blk, whole((seqs, 2048))],
        out_shape=[
            jax.ShapeDtypeStruct(state.shape, jnp.float32),
            jax.ShapeDtypeStruct((seqs, 2048), jnp.bfloat16),
        ],
        scratch_shapes=[small] * 6 + [pltpu.VMEM((8, 64, 128), jnp.float32)],
        compiler_params=pltpu.CompilerParams(
            dimension_semantics=("arbitrary",), vmem_limit_bytes=60 * 1024 * 1024
        ),
        cost_estimate=pl.CostEstimate(flops=40_000_000_000, bytes_accessed=44_000_000, transcendentals=0),
        name="attention",
    )(*ops, state)
    return new_state, part


B_N = 8
A_N = 8
HALF = 1024


def mid_kernel(
    part_ref, hid_ref, fg_ref, meta_ref, eg_ref, eu_ref, ed_ref, *rest,
):
    dw = rest[:8]
    (out_ref, pbuf, metas, tok, p_s, pst_s, wg, wu, wdn, dws, disp, xin, ybuf, ysend, yrecv, zbuf, ret, dbuf, dsend,
     drecv, rsend, rs, obuf, fres,
     s_tp, r_tp, s_meta, r_meta, s_tok, r_tok, s_fwd, r_fwd, s_dis, r_dis, s_xf, r_xf, s_y, r_y, s_ret, r_ret, s_dn, r_dn,
     s_rs, r_rs, s_out, r_out, l_w, l_d) = rest[8:]
    ep = lax.axis_index("ep")
    t = lax.axis_index("tp")
    b = ep // 8
    a = ep % 8
    mate = (ep, 1 - t)

    loads = [
        pltpu.make_async_copy(eg_ref.at[0], wg, l_w.at[0]),
        pltpu.make_async_copy(eu_ref.at[0], wu, l_w.at[1]),
        pltpu.make_async_copy(ed_ref.at[0], wdn, l_w.at[2]),
    ]
    dloads = [pltpu.make_async_copy(dw[k], dws.at[k], l_d.at[k]) for k in range(8)]

    def b_peer(k):
        return ((b + k) % 8) * 8 + a

    def a_peer(k):
        return b * 8 + (a + k) % 8

    barrier = pltpu.get_barrier_semaphore()
    pl.semaphore_signal(barrier, inc=1, device_id=mate, device_id_type=MESH)
    for k in range(1, 8):
        pl.semaphore_signal(barrier, inc=1, device_id=(b_peer(k), t), device_id_type=MESH)
        pl.semaphore_signal(barrier, inc=1, device_id=(a_peer(k), t), device_id_type=MESH)
    for c in loads + dloads:
        c.start()
    pl.semaphore_wait(barrier, 15)

    def send(src, dst, s, r, dev):
        c = pltpu.make_async_remote_copy(
            src_ref=src, dst_ref=dst, send_sem=s, recv_sem=r, device_id=dev, device_id_type=MESH
        )
        c.start()
        return c

    pending = []
    c_tp = send(part_ref, pbuf, s_tp, r_tp, mate)
    metas[b] = meta_ref[...]
    c_meta = [send(meta_ref, metas.at[b], s_meta.at[k], r_meta.at[k], (b_peer(k), t)) for k in range(1, 8)]
    c_tp.wait()
    attn = part_ref[...].astype(jnp.float32) + pbuf[...].astype(jnp.float32)
    first = (hid_ref[...].astype(jnp.float32) + attn).astype(jnp.bfloat16)
    fres[0] = first[:, :HALF]
    fres[1] = first[:, HALF:]
    f32 = first.astype(jnp.float32)
    ffn = (
        f32 * lax.rsqrt(jnp.mean(f32 * f32, axis=-1, keepdims=True) + 1e-06) * fg_ref[...]
    ).astype(jnp.bfloat16)
    mine = pl.ds(pl.multiple_of(b * 64, 64), 64)
    tok[0, mine, :] = ffn[:, :HALF]
    tok[1, mine, :] = ffn[:, HALF:]
    c_tok = [
        send(tok.at[t, mine, :], tok.at[t, mine, :], s_tok.at[k], r_tok.at[k], (b_peer(k), t)) for k in range(1, 8)
    ]

    for c in c_meta:
        c.wait()
    low = lax.broadcasted_iota(jnp.int32, (8, 128), 1) < 64
    rows = jnp.concatenate([jnp.where(low, metas[2 * i], metas[2 * i + 1]) for i in range(4)], axis=1)
    ids = (lax.broadcasted_iota(jnp.int32, (8, 512), 0) + b * 8).astype(jnp.float32)
    hit0, hit1 = rows[0:1] == ids, rows[1:2] == ids
    one0, one1 = jnp.where(hit0, 1.0, 0.0), jnp.where(hit1, 1.0, 0.0)
    hit = one0 + one1
    scale = one0 * rows[2:3] + one1 * rows[3:4]
    upper = jnp.where(
        lax.broadcasted_iota(jnp.int32, (512, 512), 0) < lax.broadcasted_iota(jnp.int32, (512, 512), 1), 1.0, 0.0
    ).astype(jnp.bfloat16)
    rank = dot(hit.astype(jnp.bfloat16), upper)
    rank = jnp.where(hit > 0.5, rank, -1.0)
    place = lax.broadcasted_iota(jnp.int32, (32, 512), 0).astype(jnp.float32)
    for j in range(8):
        same = rank[j : j + 1] == place
        p_s[pl.ds(j * 32, 32), :] = jnp.where(same, 1.0, 0.0).astype(jnp.bfloat16)
    for i in range(2):
        block = jnp.concatenate(
            [
                jnp.where(rank[j : j + 1] == place, jnp.broadcast_to(scale[j : j + 1], (32, 512)), 0.0)
                for j in range(4 * i, 4 * i + 4)
            ],
            axis=0,
        )
        pst_s[:, i * 128 : (i + 1) * 128] = block.T.astype(jnp.bfloat16)

    c_fwd = []
    for k in range(1, 8):
        c_tok[k - 1].wait()
        his = pl.ds(pl.multiple_of(((b + 8 - k) % 8) * 64, 64), 64)
        c_fwd.append(send(tok.at[t, his, :], tok.at[t, his, :], s_fwd.at[k], r_fwd.at[k], mate))

    disp[...] = dot(p_s[...], tok[t]).astype(jnp.bfloat16).reshape(8, 32, HALF)
    c_dis = [
        send(disp.at[(a + k) % 8], xin.at[t, a], s_dis.at[k], r_dis.at[k], (a_peer(k), t)) for k in range(1, 8)
    ]
    xin[t, a] = disp[a]
    c_xf = [send(disp.at[a], xin.at[t, a], s_xf.at[0], r_xf.at[0], mate)]

    for c in c_fwd:
        c.wait()
    for c in dloads:
        c.wait()
    gate = dws[:, 0].reshape(384, 2048)
    up = dws[:, 1].reshape(384, 2048)
    down = dws[:, 2].reshape(384, 2048)
    g = nt_dot(tok[0], gate[:, :HALF]) + nt_dot(tok[1], gate[:, HALF:])
    u = nt_dot(tok[0], up[:, :HALF]) + nt_dot(tok[1], up[:, HALF:])
    blend = 1.0 / (1.0 + jnp.exp(-g[:, 44:45]))
    act = (g / (1.0 + jnp.exp(-g)) * u).astype(jnp.bfloat16)
    dbuf[0] = dot(act, down[:, :HALF]) * blend
    dbuf[1] = dot(act, down[:, HALF:]) * blend
    dsend[...] = dbuf[1 - t].astype(jnp.bfloat16)
    c_dn = send(dsend, drecv, s_dn, r_dn, mate)

    for k in range(1, 8):
        c_dis[k - 1].wait()
        src = (a + 8 - k) % 8
        c_xf.append(send(xin.at[t, src], xin.at[t, src], s_xf.at[k], r_xf.at[k], mate))
    for c in loads:
        c.wait()
    for c in c_xf:
        c.wait()
    x0 = xin[0].reshape(256, HALF)
    x1 = xin[1].reshape(256, HALF)
    g = dot(x0, wg[:HALF]) + dot(x1, wg[HALF:])
    u = dot(x0, wu[:HALF]) + dot(x1, wu[HALF:])
    act = (g / (1.0 + jnp.exp(-g)) * u).astype(jnp.bfloat16)
    ybuf[0] = dot(act, wdn[:, :HALF])
    ybuf[1] = dot(act, wdn[:, HALF:])
    ysend[...] = ybuf[1 - t].astype(jnp.bfloat16)
    c_y = send(ysend, yrecv, s_y, r_y, mate)
    c_y.wait()
    zbuf[...] = (ybuf[t] + yrecv[...].astype(jnp.float32)).astype(jnp.bfloat16).reshape(8, 32, HALF)
    c_ret = [
        send(zbuf.at[(a + k) % 8], ret.at[a], s_ret.at[k], r_ret.at[k], (a_peer(k), t)) for k in range(1, 8)
    ]
    ret[a] = zbuf[a]
    c_dn.wait()
    for c in c_ret:
        c.wait()
    both = dot(pst_s[...], ret[...].reshape(256, HALF)) + dbuf[t] + drecv[...].astype(jnp.float32)
    rsend[...] = both.astype(jnp.bfloat16).reshape(8, 64, HALF)
    c_rs = [
        send(rsend.at[(b + k) % 8], rs.at[b], s_rs.at[k], r_rs.at[k], (b_peer(k), t)) for k in range(1, 8)
    ]
    rs[b] = rsend[b]
    for c in c_rs:
        c.wait()
    total = rs[0].astype(jnp.float32)
    for i in range(1, 8):
        total += rs[i].astype(jnp.float32)
    obuf[t] = (fres[t].astype(jnp.float32) + total).astype(jnp.bfloat16)
    c_out = send(obuf.at[t], obuf.at[t], s_out, r_out, mate)
    c_out.wait()
    out_ref[:, :HALF] = obuf[0]
    out_ref[:, HALF:] = obuf[1]


def middle(part, hidden, ffn_gain, meta, eg, eu, ed, dense):
    vm = pl.BlockSpec(memory_space=pltpu.VMEM)
    anyw = pl.BlockSpec(memory_space=pl.ANY)
    bf, f4 = jnp.bfloat16, jnp.float32
    dma = pltpu.SemaphoreType.DMA
    scratch = [
        pltpu.VMEM((64, 2048), bf),
        pltpu.VMEM((8, 8, 128), f4),
        pltpu.VMEM((2, 512, HALF), bf),
        pltpu.VMEM((256, 512), bf),
        pltpu.VMEM((512, 256), bf),
        pltpu.VMEM((2048, 768), bf),
        pltpu.VMEM((2048, 768), bf),
        pltpu.VMEM((768, 2048), bf),
        pltpu.VMEM((8, 3, 48, 2048), bf),
        pltpu.VMEM((8, 32, HALF), bf),
        pltpu.VMEM((2, 8, 32, HALF), bf),
        pltpu.VMEM((2, 256, HALF), f4),
        pltpu.VMEM((256, HALF), bf),
        pltpu.VMEM((256, HALF), bf),
        pltpu.VMEM((8, 32, HALF), bf),
        pltpu.VMEM((8, 32, HALF), bf),
        pltpu.VMEM((2, 512, HALF), f4),
        pltpu.VMEM((512, HALF), bf),
        pltpu.VMEM((512, HALF), bf),
        pltpu.VMEM((8, 64, HALF), bf),
        pltpu.VMEM((8, 64, HALF), bf),
        pltpu.VMEM((2, 64, HALF), bf),
        pltpu.VMEM((2, 64, HALF), bf),
        dma, dma, dma((8,)), dma((8,)), dma((8,)), dma((8,)), dma((8,)), dma((8,)), dma((8,)), dma((8,)),
        dma((8,)), dma((8,)), dma, dma, dma((8,)), dma((8,)), dma, dma, dma((8,)), dma((8,)), dma, dma,
        dma((3,)), dma((8,)),
    ]
    return pl.pallas_call(
        mid_kernel,
        out_shape=jax.ShapeDtypeStruct(hidden.shape, bf),
        in_specs=[vm] * 4 + [anyw] * 11,
        out_specs=vm,
        scratch_shapes=scratch,
        compiler_params=pltpu.CompilerParams(
            collective_id=0, has_side_effects=True, vmem_limit_bytes=62 * 1024 * 1024
        ),
        cost_estimate=pl.CostEstimate(flops=40_000_000_000, bytes_accessed=16_000_000, transcendentals=0),
        name="middle",
    )(part, hidden, ffn_gain.reshape(1, -1), meta, eg, eu, ed, *dense)


def dense_shift(dx, dy):
    pairs = []
    for ep in range(64):
        b, y, x = ep // 8, ep // 4 % 2, ep % 4
        pairs.append((ep, b * 8 + (y + dy) % 2 * 4 + (x + dx) % 4))
    return pairs


def shards(
    hidden, mix_gain, recept_weight, key_weight, value_weight, decay_down, decay_up, decay_bias, rate_down, rate_up,
    rate_bias, head_gain, out_weight, memory_state, ffn_gain, blend_vector, dense_gate, dense_up, dense_down,
    expert_gate, expert_up, expert_down, routing, route_scale,
):
    units, model = dense_down.shape
    gap = jnp.zeros((48 - units, model), jnp.bfloat16)
    gate = jnp.concatenate([dense_gate.T, blend_vector[None], gap[1:]], axis=0)
    up = jnp.concatenate([dense_up.T, gap], axis=0)
    down = jnp.concatenate([dense_down, gap], axis=0)
    own = jnp.stack([gate, up, down])
    dense = [own]
    for dy in range(2):
        for dx in range(4):
            if dx or dy:
                dense.append(lax.ppermute(own, "ep", dense_shift(dx, dy)))
    info = jnp.concatenate([routing.T.astype(jnp.float32), route_scale.T, jnp.zeros((4, 64), jnp.float32)], axis=0)
    meta = jnp.concatenate([info, info], axis=1)
    new_state, part = attention(
        hidden, mix_gain, recept_weight, key_weight, value_weight, decay_down, decay_up, decay_bias,
        rate_down, rate_up, rate_bias, head_gain, out_weight, memory_state,
    )
    layer_out = middle(part, hidden, ffn_gain, meta, expert_gate, expert_up, expert_down, dense)
    return (layer_out, new_state)


def solution(mesh):
    in_specs = (
        P("ep", None),
        P(),
        P(None, "tp"),
        P(None, "tp"),
        P(None, "tp"),
        P(),
        P(),
        P(),
        P(),
        P(),
        P(),
        P(),
        P("tp", None),
        P("ep", "tp", None, None),
        P(),
        P(),
        P(None, ("ep", "tp")),
        P(None, ("ep", "tp")),
        P(("ep", "tp"), None),
        P("ep", None, "tp"),
        P("ep", None, "tp"),
        P("ep", "tp", None),
        P("ep", None),
        P("ep", None),
    )
    out_specs = (P("ep", None), P("ep", "tp", None, None))
    return jax.shard_map(shards, mesh=mesh, in_specs=in_specs, out_specs=out_specs, check_vma=False)
```

```python
import jax
import jax.numpy as jnp
from jax import lax
from jax.experimental import pallas as pl
from jax.experimental.pallas import tpu as pltpu
from jax.sharding import PartitionSpec as P

MESH = pl.DeviceIdType.MESH
CH = 8
HALF = 1024


def dot(a, b):
    return jnp.dot(a, b, preferred_element_type=jnp.float32)


def nt_dot(a, b):
    return lax.dot_general(a, b, (((1,), (1,)), ((), ())), preferred_element_type=jnp.float32)


def iota(shape, dim):
    return lax.broadcasted_iota(jnp.int32, shape, dim)


def flag(cond, dtype=jnp.bfloat16):
    return jnp.where(cond, 1.0, 0.0).astype(dtype)


def layer_kernel(
    hid_ref, mixg_ref, dd_ref, du_ref, db_ref, rd_ref, ru_ref, rb_ref, hg_ref, fg_ref, bv_ref, dg_ref, dup_ref, ddn_ref,
    route_ref, scale_ref, wr_ref, wk_ref, wv_ref, ow_ref, st_ref, eg_ref, eu_ref, ed_ref,
    out_ref, k_s, d_s, l_s, v_s,
    wr, wk, wv, ow, st, g_s, bt_s, yt_s, part, pbuf, fres, tok, tq, pbig, pst, wg, wu, wdn, dws, disp, xin, xs, ybuf,
    ysend, yrecv, zsend, ret, dbuf, dsend, drecv, rsend, rs, obuf,
    l_a, l_s_sem, l_w, s_tp, r_tp, s_tok, r_tok, s_fwd, r_fwd, s_dis, r_dis, s_xf, r_xf, s_y, r_y, s_ret, r_ret,
    s_dn, r_dn, s_rs, r_rs, s_out, r_out, s_w, r_w,
):
    ep = lax.axis_index("ep")
    t = lax.axis_index("tp")
    b = ep // 8
    a = ep % 8
    x = ep % 4
    mate = (ep, 1 - t)
    ymate = (ep + 4 - 8 * ((ep // 4) % 2), t)
    xp = (ep - x + (x + 1) % 4, t)
    xm = (ep - x + (x + 3) % 4, t)
    heads, size = 8, 64
    width = heads * size

    def b_peer(k):
        return (((b + k) % 8) * 8 + a, t)

    barrier = pltpu.get_barrier_semaphore()
    pl.semaphore_signal(barrier, inc=1, device_id=mate, device_id_type=MESH)

    def greet(k, _):
        pl.semaphore_signal(barrier, inc=1, device_id=((ep + k) % 64, t), device_id_type=MESH)
        return 0

    lax.fori_loop(1, 64, greet, 0)

    aload = [
        pltpu.make_async_copy(src, dst, l_a.at[i])
        for i, (src, dst) in enumerate([(wk_ref, wk), (wr_ref, wr), (wv_ref, wv), (ow_ref, ow)])
    ]
    wload = [
        pltpu.make_async_copy(src.at[0], dst, l_w.at[i])
        for i, (src, dst) in enumerate([(eg_ref, wg), (eu_ref, wu), (ed_ref, wdn)])
    ]
    sload = [
        pltpu.make_async_copy(st_ref.at[pl.ds(c * CH, CH)], st.at[c % 4], l_s_sem.at[c]) for c in range(64 // CH)
    ]
    for c in aload[:3] + sload[:4] + aload[3:]:
        c.start()

    dws[0, :, 32:48, :] = jnp.zeros((3, 16, 2048), jnp.bfloat16)
    dws[0, 0, 0:44, :] = dg_ref[...]
    dws[0, 0, 44:45, :] = bv_ref[...]
    dws[0, 1, 0:44, :] = dup_ref[...]
    dws[0, 2, 0:44, :] = ddn_ref[...]

    def send(src, dst, s, r, dev):
        c = pltpu.make_async_remote_copy(
            src_ref=src, dst_ref=dst, send_sem=s, recv_sem=r, device_id=dev, device_id_type=MESH
        )
        c.start()
        return c

    pl.semaphore_wait(barrier, 64)
    first_half, second_half = pl.ds(0, HALF), pl.ds(HALF, HALF)
    w_y = send(dws.at[0], dws.at[1], s_w.at[0], r_w.at[0], ymate)
    w_xp = send(dws.at[0], dws.at[2], s_w.at[1], r_w.at[1], xp)
    w_xm = send(dws.at[0], dws.at[3], s_w.at[2], r_w.at[2], xm)

    own = pl.ds(pl.multiple_of(t * width, width), width)
    xh = hid_ref[...].astype(jnp.float32)
    nb = (xh * lax.rsqrt(jnp.mean(xh * xh, axis=-1, keepdims=True) + 1e-06) * mixg_ref[...]).astype(jnp.bfloat16)
    low = jnp.tanh(nt_dot(nb, dd_ref[...])).astype(jnp.bfloat16)
    pre = dot(low, du_ref[:, own]) + db_ref[:, own]
    dec = jnp.exp(-jnp.exp(-0.5) * (1.0 / (1.0 + jnp.exp(-pre))))
    rlow = nt_dot(nb, rd_ref[...]).astype(jnp.bfloat16)
    lr = 1.0 / (1.0 + jnp.exp(-(dot(rlow, ru_ref[:, own]) + rb_ref[:, own])))
    for c in aload[:3]:
        c.wait()
    key = dot(nb, wk[...]).astype(jnp.bfloat16).astype(jnp.float32)
    rec = dot(nb, wr[...]).astype(jnp.bfloat16).astype(jnp.float32)
    val = dot(nb, wv[...]).astype(jnp.bfloat16).astype(jnp.float32)
    for h in range(heads):
        cut = slice(h * size, (h + 1) * size)
        kh, lh, rh, vh = key[:, cut], lr[:, cut], rec[:, cut], val[:, cut]
        kn = kh * (1.0 / (jnp.sum(kh * kh, axis=-1, keepdims=True) + 1e-06))
        kl = kh * lh
        beta = jnp.sum(kl * rh, axis=-1, keepdims=True)
        k_s[h] = kn
        d_s[h] = dec[:, cut]
        l_s[h] = kl
        v_s[h] = vh
        g_s[h] = dec[:, cut] * rh - beta * kn
        bt_s[h] = beta * vh

    ids = iota((64, 64), 0).astype(jnp.float32)
    named = route_ref[...].astype(jnp.float32)
    one0, one1 = flag(named[0:1] == ids, jnp.float32), flag(named[1:2] == ids, jnp.float32)
    hit = one0 + one1
    scl = (one0 * scale_ref[0:1] + one1 * scale_ref[1:2]).astype(jnp.bfloat16)
    rank = dot(hit.astype(jnp.bfloat16), flag(iota((64, 64), 0) < iota((64, 64), 1)))
    rank = jnp.where(hit > 0.5, rank, -1.0).astype(jnp.bfloat16)
    tile = flag((iota((256, 64), 0) & 63) == iota((256, 64), 1))
    row, col = iota((1024, 256), 0), iota((1024, 256), 1)
    grown = dot(flag((iota((1024, 64), 0) >> 4) == iota((1024, 64), 1)), nt_dot(rank, tile).astype(jnp.bfloat16))
    pbig[...] = flag((grown == (row & 3).astype(jnp.float32)) & (((row >> 2) & 3) == (col >> 6)))
    row, col = iota((256, 1024), 0), iota((256, 1024), 1)
    spread = flag(iota((64, 1024), 0) == (iota((64, 1024), 1) >> 4))
    grown = dot(nt_dot(tile, rank).astype(jnp.bfloat16), spread)
    weight = dot(nt_dot(tile, scl).astype(jnp.bfloat16), spread)
    keep = (grown == (col & 3).astype(jnp.float32)) & (((col >> 2) & 3) == (row >> 6))
    pst[...] = jnp.where(keep, weight, 0.0).astype(jnp.bfloat16)

    lane = iota((size, 128), 1)
    chunks = 64 // CH
    w_2 = []
    for c in range(chunks):
        sload[c].wait()

        def one(j, _, c=c):
            for u in range(4):
                sl = j * 4 + u
                s = c * CH + sl
                for h in range(heads):
                    y = jnp.sum(st[c % 4, sl, h] * g_s[h, pl.ds(s, 1), :], axis=-1, keepdims=True)
                    yt_s[h] = jnp.where(lane == s, y, yt_s[h])
            return 0

        lax.fori_loop(0, CH // 4, one, 0)
        if c + 4 < chunks:
            sload[c + 4].start()
        if c == 3:
            for w in wload:
                w.start()
    for h in range(heads):
        y = yt_s[h].T[:64] + bt_s[h]
        cen = y - jnp.mean(y, axis=-1, keepdims=True)
        var = jnp.mean(cen * cen, axis=-1, keepdims=True)
        part[:, h * size : (h + 1) * size] = cen * lax.rsqrt(var + 0.00064)
    hn = (part[:, :width] * hg_ref[:, own]).astype(jnp.bfloat16)
    aload[3].wait()
    pbuf[0] = dot(hn, ow[...]).astype(jnp.bfloat16)
    c_tp = send(pbuf.at[0], pbuf.at[1], s_tp, r_tp, mate)
    w_y.wait()
    w_2.append(send(dws.at[1], dws.at[5], s_w.at[3], r_w.at[3], xp))
    w_2.append(send(dws.at[1], dws.at[6], s_w.at[4], r_w.at[4], xm))
    w_xp.wait()
    w_xm.wait()
    w_a = send(dws.at[2, :, :, first_half], dws.at[4, :, :, first_half], s_w.at[5], r_w.at[5], xp)
    w_b = send(dws.at[3, :, :, second_half], dws.at[4, :, :, second_half], s_w.at[6], r_w.at[6], xm)
    c_tp.wait()
    attn = pbuf[0].astype(jnp.float32) + pbuf[1].astype(jnp.float32)
    first = (hid_ref[...].astype(jnp.float32) + attn).astype(jnp.bfloat16)
    fres[0] = first[:, :HALF]
    fres[1] = first[:, HALF:]
    f32 = first.astype(jnp.float32)
    ffn = (
        f32 * lax.rsqrt(jnp.mean(f32 * f32, axis=-1, keepdims=True) + 1e-06) * fg_ref[...]
    ).astype(jnp.bfloat16)
    mine = pl.ds(pl.multiple_of(b * 64, 64), 64)
    tok[0, mine, :] = ffn[:, :HALF]
    tok[1, mine, :] = ffn[:, HALF:]
    c_tok = [send(tok.at[t, mine, :], tok.at[t, mine, :], s_tok.at[k], r_tok.at[k], b_peer(k)) for k in range(1, 8)]
    for q in range(8):
        tq[q // 4, (q % 4) * 64 : (q % 4 + 1) * 64, :] = ffn[:, q * 256 : (q + 1) * 256]
    disp[...] = dot(pbig[...], tq[t]).astype(jnp.bfloat16).reshape(64, 16, 256)

    def scatter(k, _):
        e = (ep + k) % 64
        send(disp.at[e], xin.at[t, ep], s_dis, r_dis, (e, t))
        return 0

    lax.fori_loop(1, 64, scatter, 0)
    xin[t, ep] = disp[ep]

    c_fwd = []
    for k in range(1, 8):
        c_tok[k - 1].wait()
        his = pl.ds(pl.multiple_of(((b + 8 - k) % 8) * 64, 64), 64)
        c_fwd.append(send(tok.at[t, his, :], tok.at[t, his, :], s_fwd.at[k], r_fwd.at[k], mate))
    most = pl.ds(0, 63)
    c_dis = pltpu.make_async_remote_copy(
        src_ref=disp.at[most], dst_ref=xin.at[t, most], send_sem=s_dis, recv_sem=r_dis, device_id=mate,
        device_id_type=MESH,
    )
    c_dis.wait()
    c_xf = send(xin.at[t], xin.at[t], s_xf, r_xf, mate)
    for w in w_2:
        w.wait()
    w_c = send(dws.at[5, :, :, first_half], dws.at[7, :, :, first_half], s_w.at[7], r_w.at[7], xp)
    w_d = send(dws.at[6, :, :, second_half], dws.at[7, :, :, second_half], s_w.at[8], r_w.at[8], xm)

    row, col = iota((256, 256), 0), iota((256, 256), 1)
    regroup = flag(
        (((row >> 6) == ((col >> 2) & 3)) & (((row >> 2) & 15) == (col >> 4))) & ((row & 3) == (col & 3))
    )
    ungroup = flag(
        (((col >> 6) == ((row >> 2) & 3)) & (((col >> 2) & 15) == (row >> 4))) & ((row & 3) == (col & 3))
    )
    c_xf.wait()
    for hf in range(2):
        for m in range(4):
            block = dot(regroup, xin[hf, m * 16 : (m + 1) * 16].reshape(256, 256)).astype(jnp.bfloat16)
            for q in range(4):
                xs[hf, m * 64 : (m + 1) * 64, q * 256 : (q + 1) * 256] = block[q * 64 : (q + 1) * 64]
    for w in wload:
        w.wait()
    g = dot(xs[0], wg[:HALF]) + dot(xs[1], wg[HALF:])
    u = dot(xs[0], wu[:HALF]) + dot(xs[1], wu[HALF:])
    act = (g / (1.0 + jnp.exp(-g)) * u).astype(jnp.bfloat16)
    ybuf[0] = dot(act, wdn[:, :HALF])
    ybuf[1] = dot(act, wdn[:, HALF:])
    ysend[...] = ybuf[1 - t].astype(jnp.bfloat16)
    c_y = send(ysend, yrecv, s_y, r_y, mate)
    c_y.wait()
    z = (ybuf[t] + yrecv[...].astype(jnp.float32)).astype(jnp.bfloat16)
    for m in range(4):
        block = jnp.concatenate([z[m * 64 : (m + 1) * 64, q * 256 : (q + 1) * 256] for q in range(4)], axis=0)
        zsend[m * 16 : (m + 1) * 16] = dot(ungroup, block).astype(jnp.bfloat16).reshape(16, 16, 256)

    def gather(k, _):
        e = (ep + k) % 64
        send(zsend.at[e], ret.at[ep], s_ret, r_ret, (e, t))
        return 0

    lax.fori_loop(1, 64, gather, 0)
    ret[ep] = zsend[ep]

    for c in c_fwd + [w_a, w_b, w_c, w_d]:
        c.wait()
    gate = dws[:, 0].reshape(384, 2048)
    up = dws[:, 1].reshape(384, 2048)
    down = dws[:, 2].reshape(384, 2048)
    g = nt_dot(tok[0], gate[:, :HALF]) + nt_dot(tok[1], gate[:, HALF:])
    u = nt_dot(tok[0], up[:, :HALF]) + nt_dot(tok[1], up[:, HALF:])
    blend = 1.0 / (1.0 + jnp.exp(-g[:, 44:45]))
    act = (g / (1.0 + jnp.exp(-g)) * u).astype(jnp.bfloat16)
    dbuf[0] = dot(act, down[:, :HALF]) * blend
    dbuf[1] = dot(act, down[:, HALF:]) * blend
    dsend[...] = dbuf[1 - t].astype(jnp.bfloat16)
    c_dn = send(dsend, drecv, s_dn, r_dn, mate)
    c_dn.wait()
    rsend[...] = (dbuf[t] + drecv[...].astype(jnp.float32)).astype(jnp.bfloat16).reshape(8, 64, HALF)
    c_rs = [send(rsend.at[(b + k) % 8], rs.at[b], s_rs.at[k], r_rs.at[k], b_peer(k)) for k in range(1, 8)]
    rs[b] = rsend[b]

    c_ret = pltpu.make_async_remote_copy(
        src_ref=zsend.at[most], dst_ref=ret.at[most], send_sem=s_ret, recv_sem=r_ret, device_id=mate,
        device_id_type=MESH,
    )
    c_ret.wait()
    comb = dot(pst[...], ret[...].reshape(1024, 256))
    for c in c_rs:
        c.wait()
    total = fres[t].astype(jnp.float32)
    for i in range(8):
        total += rs[i].astype(jnp.float32)
    for q in range(4):
        piece = slice(q * 256, (q + 1) * 256)
        obuf[t, :, piece] = (total[:, piece] + comb[q * 64 : (q + 1) * 64]).astype(jnp.bfloat16)
    c_out = send(obuf.at[t], obuf.at[t], s_out, r_out, mate)
    c_out.wait()
    out_ref[:, :HALF] = obuf[0]
    out_ref[:, HALF:] = obuf[1]


def layer(small, large):
    vm = pl.BlockSpec(memory_space=pltpu.VMEM)
    anyw = pl.BlockSpec(memory_space=pl.ANY)
    bf, f4 = jnp.bfloat16, jnp.float32
    dma = pltpu.SemaphoreType.DMA
    v = pltpu.VMEM
    scratch = [
        v((2048, 512), bf), v((2048, 512), bf), v((2048, 512), bf), v((512, 2048), bf),
        v((4, CH, 8, 64, 64), f4),
        v((8, 64, 64), f4), v((8, 64, 64), f4), v((8, 64, 128), f4),
        v((64, 512), f4), v((2, 64, 2048), bf), v((2, 64, HALF), bf),
        v((2, 512, HALF), bf), v((2, 256, 256), bf), v((1024, 256), bf), v((256, 1024), bf),
        v((2048, 768), bf), v((2048, 768), bf), v((768, 2048), bf),
        v((8, 3, 48, 2048), bf),
        v((64, 16, 256), bf), v((2, 64, 16, 256), bf), v((2, 256, HALF), bf),
        v((2, 256, HALF), f4), v((256, HALF), bf), v((256, HALF), bf),
        v((64, 16, 256), bf), v((64, 16, 256), bf),
        v((2, 512, HALF), f4), v((512, HALF), bf), v((512, HALF), bf),
        v((8, 64, HALF), bf), v((8, 64, HALF), bf), v((2, 64, HALF), bf),
        dma((4,)), dma((8,)), dma((3,)), dma, dma, dma((8,)), dma((8,)), dma((8,)), dma((8,)), dma, dma, dma, dma,
        dma, dma, dma, dma, dma, dma, dma((8,)), dma((8,)), dma, dma, dma((9,)), dma((9,)),
    ]
    rows = jax.ShapeDtypeStruct((8, 64, 64), f4)
    return pl.pallas_call(
        layer_kernel,
        out_shape=[jax.ShapeDtypeStruct((64, 2048), bf), rows, rows, rows, rows],
        in_specs=[vm] * len(small) + [anyw] * len(large),
        out_specs=[vm] * 5,
        scratch_shapes=scratch,
        compiler_params=pltpu.CompilerParams(
            collective_id=0, has_side_effects=True, vmem_limit_bytes=63 * 1024 * 1024
        ),
        name="layer",
    )(*small, *large)


SB = 8


def state_kernel(k_s, d_s, l_s, v_s, tokens_ref, st_ref, ns_ref, out_ref):
    step = pl.program_id(0)
    out_ref[...] = tokens_ref[...]
    eye = iota((64, 64), 0) == iota((64, 64), 1)

    def one(j, _):
        for u in range(2):
            sl = j * 2 + u
            row = pl.ds(step * SB + sl, 1)
            for h in range(8):
                m = st_ref[sl, h]
                w = jnp.sum(
                    jnp.where(eye, v_s[h, row, :], 0.0) - m * k_s[h, row, :], axis=-1, keepdims=True
                )
                ns_ref[sl, h] = m * d_s[h, row, :] + w * l_s[h, row, :]
        return 0

    lax.fori_loop(0, SB // 2, one, 0)


def new_states(k_s, d_s, l_s, v_s, tokens, state):
    fixed = pl.BlockSpec((8, 64, 64), lambda g: (0, 0, 0))
    blk = pl.BlockSpec((SB, 8, 64, 64), lambda g: (g, 0, 0, 0))
    slim = pl.BlockSpec((SB, 2048), lambda g: (g, 0))
    return pl.pallas_call(
        state_kernel,
        grid=(64 // SB,),
        in_specs=[fixed] * 4 + [slim, blk],
        out_specs=[blk, slim],
        out_shape=[
            jax.ShapeDtypeStruct(state.shape, jnp.float32),
            jax.ShapeDtypeStruct(tokens.shape, jnp.bfloat16),
        ],
        compiler_params=pltpu.CompilerParams(
            dimension_semantics=("arbitrary",), vmem_limit_bytes=40 * 1024 * 1024
        ),
        name="states",
    )(k_s, d_s, l_s, v_s, tokens, state)


def shards(
    hidden, mix_gain, recept_weight, key_weight, value_weight, decay_down, decay_up, decay_bias, rate_down, rate_up,
    rate_bias, head_gain, out_weight, memory_state, ffn_gain, blend_vector, dense_gate, dense_up, dense_down,
    expert_gate, expert_up, expert_down, routing, route_scale,
):
    flat = lambda vec: vec.reshape(1, -1)
    small = [
        hidden, flat(mix_gain), decay_down.T, decay_up, flat(decay_bias), rate_down.T, rate_up, flat(rate_bias),
        flat(head_gain), flat(ffn_gain), flat(blend_vector), dense_gate.T, dense_up.T, dense_down, routing.T,
        route_scale.T,
    ]
    large = [recept_weight, key_weight, value_weight, out_weight, memory_state, expert_gate, expert_up, expert_down]
    tokens, k_s, d_s, l_s, v_s = layer(small, large)
    new_state, layer_out = new_states(k_s, d_s, l_s, v_s, tokens, memory_state)
    return (layer_out, new_state)


def solution(mesh):
    in_specs = (
        P("ep", None),
        P(),
        P(None, "tp"),
        P(None, "tp"),
        P(None, "tp"),
        P(),
        P(),
        P(),
        P(),
        P(),
        P(),
        P(),
        P("tp", None),
        P("ep", "tp", None, None),
        P(),
        P(),
        P(None, ("ep", "tp")),
        P(None, ("ep", "tp")),
        P(("ep", "tp"), None),
        P("ep", None, "tp"),
        P("ep", None, "tp"),
        P("ep", "tp", None),
        P("ep", None),
        P("ep", None),
    )
    out_specs = (P("ep", None), P("ep", "tp", None, None))
    return jax.shard_map(shards, mesh=mesh, in_specs=in_specs, out_specs=out_specs, check_vma=False)
```

```python
import jax
import jax.numpy as jnp
from jax import lax
from jax.experimental import pallas as pl
from jax.experimental.pallas import tpu as pltpu
from jax.sharding import PartitionSpec as P

MESH = pl.DeviceIdType.MESH
CH = 8
HALF = 1024


def dot(a, b):
    return jnp.dot(a, b, preferred_element_type=jnp.float32)


def nt_dot(a, b):
    return lax.dot_general(a, b, (((1,), (1,)), ((), ())), preferred_element_type=jnp.float32)


def iota(shape, dim):
    return lax.broadcasted_iota(jnp.int32, shape, dim)


def flag(cond, dtype=jnp.bfloat16):
    return jnp.where(cond, 1.0, 0.0).astype(dtype)


def layer_kernel(
    mixg_ref, db_ref, rb_ref, hg_ref, fg_ref, bv_ref, route_ref, scale_ref,
    hid_in, dd_in, du_in, rd_in, ru_in, dg_in, dup_in, ddn_in, wr_ref, wk_ref, wv_ref, ow_ref, st_ref, eg_ref, eu_ref,
    ed_ref,
    out_ref, rows_ref,
    hid_ref, dd_ref, du_ref, rd_ref, ru_ref, dg_ref, dup_ref, ddn_ref, wr, wk, wv, ow, st, g_s, bt_s, yt_s, part, pbuf, fres, tok, tq, pbig, pst, wg, wu, wdn, dws, disp, xin, xs, ybuf,
    ysend, yrecv, zsend, ret, dbuf, dsend, drecv, rsend, rs, obuf,
    l_i, l_a, l_s_sem, l_w, s_tp, r_tp, s_tok, r_tok, s_fwd, r_fwd, s_dis, r_dis, s_xf, r_xf, s_y, r_y, s_ret, r_ret,
    s_dn, r_dn, s_rs, r_rs, s_out, r_out, s_w, r_w,
):
    ep = lax.axis_index("ep")
    t = lax.axis_index("tp")
    place = (ep % 4, (ep // 4) % 4, ep // 16)
    mate = (ep, 1 - t)
    heads, size = 8, 64
    width = heads * size

    def chip(where):
        return (where[2] * 16 + where[1] * 4 + where[0], t)

    def b_peer(k):
        return chip([(c + 2 * ((k >> d) & 1)) % 4 for d, c in enumerate(place)])

    def beside(axis):
        step = [0, 0, 0]
        step[axis] = (1 - 2 * (place[axis] % 2)) * (1 - 2 * t) + 4
        return chip([(c + o) % 4 for c, o in zip(place, step)])

    k_s, d_s, l_s, v_s = rows_ref.at[0], rows_ref.at[1], rows_ref.at[2], rows_ref.at[3]
    iload = [
        pltpu.make_async_copy(src, dst, l_i.at[i])
        for i, (src, dst) in enumerate([
            (dg_in, dg_ref), (dup_in, dup_ref), (ddn_in, ddn_ref), (hid_in, hid_ref), (dd_in, dd_ref), (du_in, du_ref),
            (rd_in, rd_ref), (ru_in, ru_ref),
        ])
    ]
    for c in iload:
        c.start()
    barrier = pltpu.get_barrier_semaphore()
    pl.semaphore_signal(barrier, inc=1, device_id=mate, device_id_type=MESH)

    def greet(k, _):
        pl.semaphore_signal(barrier, inc=1, device_id=((ep + k) % 64, t), device_id_type=MESH)
        return 0

    lax.fori_loop(1, 64, greet, 0)

    aload = [
        pltpu.make_async_copy(src, dst, l_a.at[i])
        for i, (src, dst) in enumerate([(wk_ref, wk), (wr_ref, wr), (wv_ref, wv), (ow_ref, ow)])
    ]
    wload = [
        pltpu.make_async_copy(src.at[0], dst, l_w.at[i])
        for i, (src, dst) in enumerate([(eg_ref, wg), (eu_ref, wu), (ed_ref, wdn)])
    ]
    sload = [
        pltpu.make_async_copy(st_ref.at[pl.ds(c * CH, CH)], st.at[c % 4], l_s_sem.at[c]) for c in range(64 // CH)
    ]
    for c in aload[:3] + sload[:4] + aload[3:]:
        c.start()

    for c in iload:
        c.wait()
    dws[0, :, 32:48, :] = jnp.zeros((3, 16, 2048), jnp.bfloat16)
    dws[0, 0, 0:44, :] = dg_ref[...]
    bv = bv_ref[...].astype(jnp.float32)
    dws[0, 0, 44:45, :] = jnp.concatenate([bv[i : i + 1] for i in range(16)], axis=1).astype(jnp.bfloat16)
    dws[0, 1, 0:44, :] = dup_ref[...]
    dws[0, 2, 0:44, :] = ddn_ref[...]

    def send(src, dst, s, r, dev):
        c = pltpu.make_async_remote_copy(
            src_ref=src, dst_ref=dst, send_sem=s, recv_sem=r, device_id=dev, device_id_type=MESH
        )
        c.start()
        return c

    pl.semaphore_wait(barrier, 64)

    def leg(n):
        copies = []
        for m in range(3):
            axes = [(m + i) % 3 for i in range(3)]
            for mask in range(1 << n):
                held = sum(1 << axes[i] for i in range(n) if mask >> i & 1)
                then = held + (1 << axes[n])
                sem = m * 8 + then
                copies.append(send(dws.at[held, m], dws.at[then, m], s_w.at[sem], r_w.at[sem], beside(axes[n])))
        return copies

    legs = leg(0)

    own = pl.ds(pl.multiple_of(t * width, width), width)
    xh = hid_ref[...].astype(jnp.float32)
    nb = (xh * lax.rsqrt(jnp.mean(xh * xh, axis=-1, keepdims=True) + 1e-06) * mixg_ref[...]).astype(jnp.bfloat16)
    low = jnp.tanh(nt_dot(nb, dd_ref[...])).astype(jnp.bfloat16)
    pre = dot(low, du_ref[:, own]) + db_ref[:, own]
    dec = jnp.exp(-jnp.exp(-0.5) * (1.0 / (1.0 + jnp.exp(-pre))))
    rlow = nt_dot(nb, rd_ref[...]).astype(jnp.bfloat16)
    lr = 1.0 / (1.0 + jnp.exp(-(dot(rlow, ru_ref[:, own]) + rb_ref[:, own])))
    for c in aload[:3]:
        c.wait()
    key = dot(nb, wk[...]).astype(jnp.bfloat16).astype(jnp.float32)
    rec = dot(nb, wr[...]).astype(jnp.bfloat16).astype(jnp.float32)
    val = dot(nb, wv[...]).astype(jnp.bfloat16).astype(jnp.float32)
    for h in range(heads):
        cut = slice(h * size, (h + 1) * size)
        kh, lh, rh, vh = key[:, cut], lr[:, cut], rec[:, cut], val[:, cut]
        kn = kh * (1.0 / (jnp.sum(kh * kh, axis=-1, keepdims=True) + 1e-06))
        kl = kh * lh
        beta = jnp.sum(kl * rh, axis=-1, keepdims=True)
        k_s[h] = kn
        d_s[h] = dec[:, cut]
        l_s[h] = kl
        v_s[h] = vh
        g_s[h] = dec[:, cut] * rh - beta * kn
        bt_s[h] = beta * vh

    ids = iota((64, 64), 0).astype(jnp.float32)
    named = route_ref[...].astype(jnp.float32)
    one0, one1 = flag(named[0:1] == ids, jnp.float32), flag(named[1:2] == ids, jnp.float32)
    hit = one0 + one1
    scl = (one0 * scale_ref[0:1] + one1 * scale_ref[1:2]).astype(jnp.bfloat16)
    rank = dot(hit.astype(jnp.bfloat16), flag(iota((64, 64), 0) < iota((64, 64), 1)))
    rank = jnp.where(hit > 0.5, rank, -1.0).astype(jnp.bfloat16)
    tile = flag((iota((256, 64), 0) & 63) == iota((256, 64), 1))
    row, col = iota((1024, 256), 0), iota((1024, 256), 1)
    grown = dot(flag((iota((1024, 64), 0) >> 4) == iota((1024, 64), 1)), nt_dot(rank, tile).astype(jnp.bfloat16))
    pbig[...] = flag((grown == (row & 3).astype(jnp.float32)) & (((row >> 2) & 3) == (col >> 6)))
    row, col = iota((256, 1024), 0), iota((256, 1024), 1)
    spread = flag(iota((64, 1024), 0) == (iota((64, 1024), 1) >> 4))
    grown = dot(nt_dot(tile, rank).astype(jnp.bfloat16), spread)
    weight = dot(nt_dot(tile, scl).astype(jnp.bfloat16), spread)
    keep = (grown == (col & 3).astype(jnp.float32)) & (((col >> 2) & 3) == (row >> 6))
    pst[...] = jnp.where(keep, weight, 0.0).astype(jnp.bfloat16)

    for w in legs:
        w.wait()
    legs = leg(1)

    lane = iota((size, 128), 1)
    chunks = 64 // CH
    for c in range(chunks):
        sload[c].wait()

        def one(j, _, c=c):
            for u in range(4):
                sl = j * 4 + u
                s = c * CH + sl
                for h in range(heads):
                    y = jnp.sum(st[c % 4, sl, h] * g_s[h, pl.ds(s, 1), :], axis=-1, keepdims=True)
                    yt_s[h] = jnp.where(lane == s, y, yt_s[h])
            return 0

        lax.fori_loop(0, CH // 4, one, 0)
        if c + 4 < chunks:
            sload[c + 4].start()
        if c == 3:
            for w in wload:
                w.start()
        if c == 5:
            for w in legs:
                w.wait()
            legs = leg(2)
    for h in range(heads):
        y = yt_s[h].T[:64] + bt_s[h]
        cen = y - jnp.mean(y, axis=-1, keepdims=True)
        var = jnp.mean(cen * cen, axis=-1, keepdims=True)
        part[:, h * size : (h + 1) * size] = cen * lax.rsqrt(var + 0.00064)
    hn = (part[:, :width] * hg_ref[:, own]).astype(jnp.bfloat16)
    aload[3].wait()
    pbuf[0] = dot(hn, ow[...]).astype(jnp.bfloat16)
    c_tp = send(pbuf.at[0], pbuf.at[1], s_tp, r_tp, mate)
    c_tp.wait()
    attn = pbuf[0].astype(jnp.float32) + pbuf[1].astype(jnp.float32)
    first = (hid_ref[...].astype(jnp.float32) + attn).astype(jnp.bfloat16)
    fres[0] = first[:, :HALF]
    fres[1] = first[:, HALF:]
    f32 = first.astype(jnp.float32)
    ffn = (
        f32 * lax.rsqrt(jnp.mean(f32 * f32, axis=-1, keepdims=True) + 1e-06) * fg_ref[...]
    ).astype(jnp.bfloat16)
    tok[0, 0:64, :] = ffn[:, :HALF]
    tok[1, 0:64, :] = ffn[:, HALF:]
    for q in range(8):
        tq[q // 4, (q % 4) * 64 : (q % 4 + 1) * 64, :] = ffn[:, q * 256 : (q + 1) * 256]
    disp[...] = dot(pbig[...], tq[t]).astype(jnp.bfloat16).reshape(64, 16, 256)

    def scatter(k, _):
        e = (ep + k) % 64
        send(disp.at[e], xin.at[t, ep], s_dis, r_dis, (e, t))
        return 0

    lax.fori_loop(1, 64, scatter, 0)
    xin[t, ep] = disp[ep]
    c_tok = [
        send(tok.at[t, pl.ds(0, 64), :], tok.at[t, pl.ds(k * 64, 64), :], s_tok.at[k], r_tok.at[k], b_peer(k))
        for k in range(1, 8)
    ]

    most = pl.ds(0, 63)
    c_dis = pltpu.make_async_remote_copy(
        src_ref=disp.at[most], dst_ref=xin.at[t, most], send_sem=s_dis, recv_sem=r_dis, device_id=mate,
        device_id_type=MESH,
    )
    c_dis.wait()
    c_xf = send(xin.at[t], xin.at[t], s_xf, r_xf, mate)
    row, col = iota((256, 256), 0), iota((256, 256), 1)
    regroup = flag(
        (((row >> 6) == ((col >> 2) & 3)) & (((row >> 2) & 15) == (col >> 4))) & ((row & 3) == (col & 3))
    )
    ungroup = flag(
        (((col >> 6) == ((row >> 2) & 3)) & (((col >> 2) & 15) == (row >> 4))) & ((row & 3) == (col & 3))
    )
    c_xf.wait()
    for hf in range(2):
        for m in range(4):
            block = dot(regroup, xin[hf, m * 16 : (m + 1) * 16].reshape(256, 256)).astype(jnp.bfloat16)
            for q in range(4):
                xs[hf, m * 64 : (m + 1) * 64, q * 256 : (q + 1) * 256] = block[q * 64 : (q + 1) * 64]
    for w in wload:
        w.wait()
    g = dot(xs[0], wg[:HALF]) + dot(xs[1], wg[HALF:])
    u = dot(xs[0], wu[:HALF]) + dot(xs[1], wu[HALF:])
    act = (g / (1.0 + jnp.exp(-g)) * u).astype(jnp.bfloat16)
    ybuf[0] = dot(act, wdn[:, :HALF])
    ybuf[1] = dot(act, wdn[:, HALF:])
    ysend[...] = ybuf[1 - t].astype(jnp.bfloat16)
    c_y = send(ysend, yrecv, s_y, r_y, mate)
    c_fwd = []
    for k in range(1, 8):
        c_tok[k - 1].wait()
        his = pl.ds(k * 64, 64)
        c_fwd.append(send(tok.at[t, his, :], tok.at[t, his, :], s_fwd.at[k], r_fwd.at[k], mate))

    c_y.wait()
    z = (ybuf[t] + yrecv[...].astype(jnp.float32)).astype(jnp.bfloat16)
    for m in range(4):
        block = jnp.concatenate([z[m * 64 : (m + 1) * 64, q * 256 : (q + 1) * 256] for q in range(4)], axis=0)
        zsend[m * 16 : (m + 1) * 16] = dot(ungroup, block).astype(jnp.bfloat16).reshape(16, 16, 256)

    def gather(k, _):
        e = (ep + k) % 64
        send(zsend.at[e], ret.at[ep], s_ret, r_ret, (e, t))
        return 0

    lax.fori_loop(1, 64, gather, 0)
    ret[ep] = zsend[ep]

    for c in legs + c_fwd:
        c.wait()
    gate = dws[:, 0].reshape(384, 2048)
    up = dws[:, 1].reshape(384, 2048)
    down = dws[:, 2].reshape(384, 2048)
    c_dn = []
    for p in range(2):
        part_rows = slice(p * 256, p * 256 + 256)
        t0, t1 = tok[0, part_rows, :], tok[1, part_rows, :]
        g = nt_dot(t0, gate[:, :HALF]) + nt_dot(t1, gate[:, HALF:])
        u = nt_dot(t0, up[:, :HALF]) + nt_dot(t1, up[:, HALF:])
        blend = 1.0 / (1.0 + jnp.exp(-g[:, 44:45]))
        act = (g / (1.0 + jnp.exp(-g)) * u).astype(jnp.bfloat16)
        dbuf[p, 0] = dot(act, down[:, :HALF]) * blend
        dbuf[p, 1] = dot(act, down[:, HALF:]) * blend
        dsend[p] = dbuf[p, 1 - t].astype(jnp.bfloat16)
        c_dn.append(send(dsend.at[p], drecv.at[p], s_dn.at[p], r_dn.at[p], mate))
    c_rs = []
    for p in range(2):
        c_dn[p].wait()
        rsend[p * 4 : p * 4 + 4] = (
            (dbuf[p, t] + drecv[p].astype(jnp.float32)).astype(jnp.bfloat16).reshape(4, 64, HALF)
        )
        for k in range(p * 4, p * 4 + 4):
            if k:
                c_rs.append(send(rsend.at[k], rs.at[k], s_rs.at[k], r_rs.at[k], b_peer(k)))

    c_ret = pltpu.make_async_remote_copy(
        src_ref=zsend.at[most], dst_ref=ret.at[most], send_sem=s_ret, recv_sem=r_ret, device_id=mate,
        device_id_type=MESH,
    )
    c_ret.wait()
    comb = dot(pst[...], ret[...].reshape(1024, 256))
    for c in c_rs:
        c.wait()
    total = fres[t].astype(jnp.float32) + rsend[0].astype(jnp.float32)
    for i in range(1, 8):
        total += rs[i].astype(jnp.float32)
    for q in range(4):
        piece = slice(q * 256, (q + 1) * 256)
        obuf[t, :, piece] = (total[:, piece] + comb[q * 64 : (q + 1) * 64]).astype(jnp.bfloat16)
    c_out = send(obuf.at[t], obuf.at[t], s_out, r_out, mate)
    c_out.wait()
    out_ref[:, :HALF] = obuf[0]
    out_ref[:, HALF:] = obuf[1]


def layer(small, large):
    vm = pl.BlockSpec(memory_space=pltpu.VMEM)
    anyw = pl.BlockSpec(memory_space=pl.ANY)
    bf, f4 = jnp.bfloat16, jnp.float32
    dma = pltpu.SemaphoreType.DMA
    v = pltpu.VMEM
    scratch = [v(ref.shape, bf) for ref in large[:8]] + [
        v((2048, 512), bf), v((2048, 512), bf), v((2048, 512), bf), v((512, 2048), bf),
        v((4, CH, 8, 64, 64), f4),
        v((8, 64, 64), f4), v((8, 64, 64), f4), v((8, 64, 128), f4),
        v((64, 512), f4), v((2, 64, 2048), bf), v((2, 64, HALF), bf),
        v((2, 512, HALF), bf), v((2, 256, 256), bf), v((1024, 256), bf), v((256, 1024), bf),
        v((2048, 768), bf), v((2048, 768), bf), v((768, 2048), bf),
        v((8, 3, 48, 2048), bf),
        v((64, 16, 256), bf), v((2, 64, 16, 256), bf), v((2, 256, HALF), bf),
        v((2, 256, HALF), f4), v((256, HALF), bf), v((256, HALF), bf),
        v((64, 16, 256), bf), v((64, 16, 256), bf),
        v((2, 2, 256, HALF), f4), v((2, 256, HALF), bf), v((2, 256, HALF), bf),
        v((8, 64, HALF), bf), v((8, 64, HALF), bf), v((2, 64, HALF), bf),
        dma((8,)), dma((4,)), dma((8,)), dma((3,)), dma, dma, dma((8,)), dma((8,)), dma((8,)), dma((8,)), dma, dma, dma,
        dma, dma, dma, dma, dma, dma((2,)), dma((2,)), dma((8,)), dma((8,)), dma, dma, dma((24,)), dma((24,)),
    ]
    return pl.pallas_call(
        layer_kernel,
        out_shape=[jax.ShapeDtypeStruct((64, 2048), bf), jax.ShapeDtypeStruct((4, 8, 64, 64), f4)],
        in_specs=[vm] * len(small) + [anyw] * len(large),
        out_specs=[vm] * 2,
        scratch_shapes=scratch,
        compiler_params=pltpu.CompilerParams(
            collective_id=0, has_side_effects=True, vmem_limit_bytes=63 * 1024 * 1024
        ),
        name="layer",
    )(*small, *large)


SB = 4


def state_kernel(rows_ref, tokens_ref, st_ref, ns_ref, out_ref, old, new, l_in, l_out):
    count = st_ref.shape[0] // SB

    def load(c):
        own = pl.ds(c * SB, SB)
        return pltpu.make_async_copy(st_ref.at[own], old.at[own], l_in.at[c])

    def store(c):
        own = pl.ds(c * SB, SB)
        return pltpu.make_async_copy(new.at[own], ns_ref.at[own], l_out.at[c])

    for c in range(count):
        load(c).start()
    out_ref[...] = tokens_ref[...]
    eye = iota((64, 64), 0) == iota((64, 64), 1)

    def one(c, _):
        load(c).wait()
        for u in range(SB):
            s = c * SB + u
            row = pl.ds(s, 1)
            for h in range(8):
                m = old[s, h]
                w = jnp.sum(
                    jnp.where(eye, rows_ref[3, h, row, :], 0.0) - m * rows_ref[0, h, row, :], axis=-1, keepdims=True
                )
                new[s, h] = m * rows_ref[1, h, row, :] + w * rows_ref[2, h, row, :]
        store(c).start()
        return 0

    lax.fori_loop(0, count, one, 0)

    def drain(c, _):
        store(c).wait()
        return 0

    lax.fori_loop(0, count, drain, 0)


def new_states(rows, tokens, state):
    vm = pl.BlockSpec(memory_space=pltpu.VMEM)
    anyw = pl.BlockSpec(memory_space=pl.ANY)
    return pl.pallas_call(
        state_kernel,
        in_specs=[vm, vm, anyw],
        out_specs=[anyw, vm],
        out_shape=[
            jax.ShapeDtypeStruct(state.shape, jnp.float32),
            jax.ShapeDtypeStruct(tokens.shape, jnp.bfloat16),
        ],
        scratch_shapes=[
            pltpu.VMEM(state.shape, jnp.float32),
            pltpu.VMEM(state.shape, jnp.float32),
            pltpu.SemaphoreType.DMA((state.shape[0] // SB,)),
            pltpu.SemaphoreType.DMA((state.shape[0] // SB,)),
        ],
        compiler_params=pltpu.CompilerParams(vmem_limit_bytes=63 * 1024 * 1024),
        name="states",
    )(rows, tokens, state)


def shards(
    hidden, mix_gain, recept_weight, key_weight, value_weight, decay_down, decay_up, decay_bias, rate_down, rate_up,
    rate_bias, head_gain, out_weight, memory_state, ffn_gain, blend_vector, dense_gate, dense_up, dense_down,
    expert_gate, expert_up, expert_down, routing, route_scale,
):
    flat = lambda vec: vec.reshape(1, -1)
    small = [
        flat(mix_gain), flat(decay_bias), flat(rate_bias), flat(head_gain), flat(ffn_gain), blend_vector.reshape(16, 128),
        routing.T, route_scale.T,
    ]
    large = [
        hidden, decay_down.T, decay_up, rate_down.T, rate_up, dense_gate.T, dense_up.T, dense_down,
        recept_weight, key_weight, value_weight, out_weight, memory_state, expert_gate, expert_up, expert_down,
    ]
    tokens, rows = layer(small, large)
    new_state, layer_out = new_states(rows, tokens, memory_state)
    return (layer_out, new_state)


def solution(mesh):
    in_specs = (
        P("ep", None),
        P(),
        P(None, "tp"),
        P(None, "tp"),
        P(None, "tp"),
        P(),
        P(),
        P(),
        P(),
        P(),
        P(),
        P(),
        P("tp", None),
        P("ep", "tp", None, None),
        P(),
        P(),
        P(None, ("ep", "tp")),
        P(None, ("ep", "tp")),
        P(("ep", "tp"), None),
        P("ep", None, "tp"),
        P("ep", None, "tp"),
        P("ep", "tp", None),
        P("ep", None),
        P("ep", None),
    )
    out_specs = (P("ep", None), P("ep", "tp", None, None))
    return jax.shard_map(shards, mesh=mesh, in_specs=in_specs, out_specs=out_specs, check_vma=False)
```

```python
import jax
import jax.numpy as jnp
from jax import lax
from jax.experimental import pallas as pl
from jax.experimental.pallas import tpu as pltpu
from jax.sharding import PartitionSpec as P

MESH = pl.DeviceIdType.MESH
CH = 8
HALF = 1024


def dot(a, b):
    return jnp.dot(a, b, preferred_element_type=jnp.float32)


def nt_dot(a, b):
    return lax.dot_general(a, b, (((1,), (1,)), ((), ())), preferred_element_type=jnp.float32)


def iota(shape, dim):
    return lax.broadcasted_iota(jnp.int32, shape, dim)


def flag(cond, dtype=jnp.bfloat16):
    return jnp.where(cond, 1.0, 0.0).astype(dtype)


def layer_kernel(
    mixg_ref, db_ref, rb_ref, hg_ref, fg_ref, bv_ref, route_ref, scale_ref,
    hid_in, dd_in, du_in, rd_in, ru_in, dg_in, dup_in, ddn_in, wr_ref, wk_ref, wv_ref, ow_ref, st_ref, eg_ref, eu_ref,
    ed_ref,
    out_ref, ns_ref,
    rows_ref, nsb, hid_ref, dd_ref, du_ref, rd_ref, ru_ref, dg_ref, dup_ref, ddn_ref, wr, wk, wv, ow, st, g_s, bt_s, yt_s, part, pbuf, fres, tok, tq, pbig, pst, wg, wu, wdn, dws, disp, xin, xs, ybuf,
    ysend, yrecv, zsend, ret, dbuf, dsend, drecv, rsend, rs, rs2, obuf,
    l_i, l_again, l_ns, l_a, l_s_sem, l_w, s_tp, r_tp, s_tok, r_tok, s_fwd, r_fwd, s_dis, r_dis, s_xf, r_xf, s_y, r_y, s_ret, r_ret,
    s_dn, r_dn, s_rs, r_rs, s_out, r_out, s_w, r_w,
):
    ep = lax.axis_index("ep")
    t = lax.axis_index("tp")
    place = (ep % 4, (ep // 4) % 4, ep // 16)
    mate = (ep, 1 - t)
    heads, size = 8, 64
    width = heads * size

    def chip(where):
        return (where[2] * 16 + where[1] * 4 + where[0], t)

    def b_peer(k):
        return chip([(c + 2 * ((k >> d) & 1)) % 4 for d, c in enumerate(place)])

    def beside(axis):
        step = [0, 0, 0]
        step[axis] = (1 - 2 * (place[axis] % 2)) * (1 - 2 * t) + 4
        return chip([(c + o) % 4 for c, o in zip(place, step)])

    k_s, d_s, l_s, v_s = rows_ref.at[0], rows_ref.at[1], rows_ref.at[2], rows_ref.at[3]
    iload = [
        pltpu.make_async_copy(src, dst, l_i.at[i])
        for i, (src, dst) in enumerate([
            (dg_in, dg_ref), (dup_in, dup_ref), (ddn_in, ddn_ref), (hid_in, hid_ref), (dd_in, dd_ref), (du_in, du_ref),
            (rd_in, rd_ref), (ru_in, ru_ref),
        ])
    ]
    for c in iload:
        c.start()
    barrier = pltpu.get_barrier_semaphore()
    pl.semaphore_signal(barrier, inc=1, device_id=mate, device_id_type=MESH)

    def greet(k, _):
        pl.semaphore_signal(barrier, inc=1, device_id=((ep + k) % 64, t), device_id_type=MESH)
        return 0

    lax.fori_loop(1, 64, greet, 0)

    aload = [
        pltpu.make_async_copy(src, dst, l_a.at[i])
        for i, (src, dst) in enumerate([(wk_ref, wk), (wr_ref, wr), (wv_ref, wv), (ow_ref, ow)])
    ]
    wload = [
        pltpu.make_async_copy(src.at[0], dst, l_w.at[i])
        for i, (src, dst) in enumerate([(eg_ref, wg), (eu_ref, wu), (ed_ref, wdn)])
    ]
    sload = [
        pltpu.make_async_copy(st_ref.at[pl.ds(c * CH, CH)], st.at[c % 4], l_s_sem.at[c]) for c in range(64 // CH)
    ]
    for c in aload[:3] + sload[:4] + aload[3:]:
        c.start()

    ids = iota((64, 64), 0).astype(jnp.float32)
    named = route_ref[...].astype(jnp.float32)
    one0, one1 = flag(named[0:1] == ids, jnp.float32), flag(named[1:2] == ids, jnp.float32)
    hit = one0 + one1
    scl = (one0 * scale_ref[0:1] + one1 * scale_ref[1:2]).astype(jnp.bfloat16)
    rank = dot(hit.astype(jnp.bfloat16), flag(iota((64, 64), 0) < iota((64, 64), 1)))
    rank = jnp.where(hit > 0.5, rank, -1.0).astype(jnp.bfloat16)
    tile = flag((iota((256, 64), 0) & 63) == iota((256, 64), 1))
    row, col = iota((1024, 256), 0), iota((1024, 256), 1)
    grown = dot(flag((iota((1024, 64), 0) >> 4) == iota((1024, 64), 1)), nt_dot(rank, tile).astype(jnp.bfloat16))
    pbig[...] = flag((grown == (row & 3).astype(jnp.float32)) & (((row >> 2) & 3) == (col >> 6)))
    row, col = iota((256, 1024), 0), iota((256, 1024), 1)
    spread = flag(iota((64, 1024), 0) == (iota((64, 1024), 1) >> 4))
    grown = dot(nt_dot(tile, rank).astype(jnp.bfloat16), spread)
    weight = dot(nt_dot(tile, scl).astype(jnp.bfloat16), spread)
    keep = (grown == (col & 3).astype(jnp.float32)) & (((col >> 2) & 3) == (row >> 6))
    pst[...] = jnp.where(keep, weight, 0.0).astype(jnp.bfloat16)

    for c in iload:
        c.wait()
    dws[0, :, 32:48, :] = jnp.zeros((3, 16, 2048), jnp.bfloat16)
    dws[0, 0, 0:44, :] = dg_ref[...]
    bv = bv_ref[...].astype(jnp.float32)
    dws[0, 0, 44:45, :] = jnp.concatenate([bv[i : i + 1] for i in range(16)], axis=1).astype(jnp.bfloat16)
    dws[0, 1, 0:44, :] = dup_ref[...]
    dws[0, 2, 0:44, :] = ddn_ref[...]

    def send(src, dst, s, r, dev):
        c = pltpu.make_async_remote_copy(
            src_ref=src, dst_ref=dst, send_sem=s, recv_sem=r, device_id=dev, device_id_type=MESH
        )
        c.start()
        return c

    pl.semaphore_wait(barrier, 64)

    def hop(m, held, axis):
        then = held + (1 << axis)
        sem = m * 8 + then
        return send(dws.at[held, m], dws.at[then, m], s_w.at[sem], r_w.at[sem], beside(axis))

    order = [[(m + i) % 3 for i in range(3)] for m in range(3)]
    legs = []
    leg_a = [hop(m, 0, order[m][0]) for m in range(3)]
    leg_b = [hop(m, 0, order[m][1]) for m in range(3)]
    legs += [hop(m, 0, order[m][2]) for m in range(3)]

    own = pl.ds(pl.multiple_of(t * width, width), width)
    xh = hid_ref[...].astype(jnp.float32)
    nb = (xh * lax.rsqrt(jnp.mean(xh * xh, axis=-1, keepdims=True) + 1e-06) * mixg_ref[...]).astype(jnp.bfloat16)
    low = jnp.tanh(nt_dot(nb, dd_ref[...])).astype(jnp.bfloat16)
    pre = dot(low, du_ref[:, own]) + db_ref[:, own]
    dec = jnp.exp(-jnp.exp(-0.5) * (1.0 / (1.0 + jnp.exp(-pre))))
    rlow = nt_dot(nb, rd_ref[...]).astype(jnp.bfloat16)
    lr = 1.0 / (1.0 + jnp.exp(-(dot(rlow, ru_ref[:, own]) + rb_ref[:, own])))
    for c in aload[:3]:
        c.wait()
    key = dot(nb, wk[...]).astype(jnp.bfloat16).astype(jnp.float32)
    rec = dot(nb, wr[...]).astype(jnp.bfloat16).astype(jnp.float32)
    val = dot(nb, wv[...]).astype(jnp.bfloat16).astype(jnp.float32)
    for h in range(heads):
        cut = slice(h * size, (h + 1) * size)
        kh, lh, rh, vh = key[:, cut], lr[:, cut], rec[:, cut], val[:, cut]
        kn = kh * (1.0 / (jnp.sum(kh * kh, axis=-1, keepdims=True) + 1e-06))
        kl = kh * lh
        beta = jnp.sum(kl * rh, axis=-1, keepdims=True)
        k_s[h] = kn
        d_s[h] = dec[:, cut]
        l_s[h] = kl
        v_s[h] = vh
        g_s[h] = dec[:, cut] * rh - beta * kn
        bt_s[h] = beta * vh

    for w in leg_a:
        w.wait()
    leg_c = [hop(m, 1 << order[m][0], order[m][1]) for m in range(3)]
    legs += [hop(m, 1 << order[m][0], order[m][2]) for m in range(3)]
    for w in leg_b:
        w.wait()
    legs += [hop(m, 1 << order[m][1], order[m][2]) for m in range(3)]

    lane = iota((size, 128), 1)
    chunks = 64 // CH
    for c in range(chunks):
        sload[c].wait()

        def one(j, _, c=c):
            for u in range(4):
                sl = j * 4 + u
                s = c * CH + sl
                for h in range(heads):
                    y = jnp.sum(st[c % 4, sl, h] * g_s[h, pl.ds(s, 1), :], axis=-1, keepdims=True)
                    yt_s[h] = jnp.where(lane == s, y, yt_s[h])
            return 0

        lax.fori_loop(0, CH // 4, one, 0)
        if c + 4 < chunks:
            sload[c + 4].start()
        if c == 3:
            for w in wload:
                w.start()
    eye = iota((size, size), 0) == iota((size, size), 1)
    again = [
        pltpu.make_async_copy(st_ref.at[pl.ds(c * CH, CH)], st.at[c % 4], l_again.at[c]) for c in range(4)
    ]
    stores = [
        pltpu.make_async_copy(nsb.at[n % 2], ns_ref.at[pl.ds((n + 4) % 8 * CH, CH)], l_ns.at[n]) for n in range(8)
    ]

    def update(n):
        c = (n + 4) % 8
        if n >= 4:
            again[c].wait()
        if n >= 2:
            stores[n - 2].wait()

        def one(j, _):
            for u in range(4):
                sl = j * 4 + u
                at = pl.ds(c * CH + sl, 1)
                for h in range(heads):
                    m = st[c % 4, sl, h]
                    w = jnp.sum(jnp.where(eye, v_s[h, at, :], 0.0) - m * k_s[h, at, :], axis=-1, keepdims=True)
                    nsb[n % 2, sl, h] = (m * d_s[h, at, :] + w * l_s[h, at, :]).astype(jnp.bfloat16)
            return 0

        lax.fori_loop(0, CH // 4, one, 0)
        stores[n].start()
        if n < 4:
            again[n].start()

    for h in range(heads):
        y = yt_s[h].T[:64] + bt_s[h]
        cen = y - jnp.mean(y, axis=-1, keepdims=True)
        var = jnp.mean(cen * cen, axis=-1, keepdims=True)
        part[:, h * size : (h + 1) * size] = cen * lax.rsqrt(var + 0.00064)
    hn = (part[:, :width] * hg_ref[:, own]).astype(jnp.bfloat16)
    aload[3].wait()
    pbuf[0] = dot(hn, ow[...]).astype(jnp.bfloat16)
    c_tp = send(pbuf.at[0], pbuf.at[1], s_tp, r_tp, mate)
    c_tp.wait()
    attn = pbuf[0].astype(jnp.float32) + pbuf[1].astype(jnp.float32)
    first = (hid_ref[...].astype(jnp.float32) + attn).astype(jnp.bfloat16)
    fres[0] = first[:, :HALF]
    fres[1] = first[:, HALF:]
    f32 = first.astype(jnp.float32)
    ffn = (
        f32 * lax.rsqrt(jnp.mean(f32 * f32, axis=-1, keepdims=True) + 1e-06) * fg_ref[...]
    ).astype(jnp.bfloat16)
    tok[0, 0:64, :] = ffn[:, :HALF]
    tok[1, 0:64, :] = ffn[:, HALF:]
    pieces = [(0, 384), (384, 384), (768, 256)]

    def pass_on(m, held, axis):
        then = held + (1 << axis)
        cols = pl.ds(*pieces[m])
        sem = m * 8 + then
        return send(
            tok.at[t, pl.ds(held * 64, 64), cols], tok.at[t, pl.ds(then * 64, 64), cols], s_tok.at[sem], r_tok.at[sem],
            b_peer(1 << axis),
        )

    tok_a = [pass_on(m, 0, order[m][0]) for m in range(3)]
    tok_b = [pass_on(m, 0, order[m][1]) for m in range(3)]
    toks = [pass_on(m, 0, order[m][2]) for m in range(3)]
    for q in range(8):
        tq[q // 4, (q % 4) * 64 : (q % 4 + 1) * 64, :] = ffn[:, q * 256 : (q + 1) * 256]
    disp[...] = dot(pbig[...], tq[t]).astype(jnp.bfloat16).reshape(64, 16, 256)

    def scatter(k, _):
        e = (ep + k) % 64
        send(disp.at[e], xin.at[t, ep], s_dis, r_dis, (e, t))
        return 0

    lax.fori_loop(1, 64, scatter, 0)
    xin[t, ep] = disp[ep]
    for n in range(3):
        update(n)
    for c in tok_a:
        c.wait()
    tok_c = [pass_on(m, 1 << order[m][0], order[m][1]) for m in range(3)]
    toks += [pass_on(m, 1 << order[m][0], order[m][2]) for m in range(3)]
    for c in tok_b:
        c.wait()
    toks += [pass_on(m, 1 << order[m][1], order[m][2]) for m in range(3)]
    for n in range(3, 6):
        update(n)
    for c in tok_c:
        c.wait()
    toks += [pass_on(m, (1 << order[m][0]) + (1 << order[m][1]), order[m][2]) for m in range(3)]
    for w in leg_c:
        w.wait()
    legs += [hop(m, (1 << order[m][0]) + (1 << order[m][1]), order[m][2]) for m in range(3)]
    for n in range(6, 8):
        update(n)
    most = pl.ds(0, 63)
    c_dis = pltpu.make_async_remote_copy(
        src_ref=disp.at[most], dst_ref=xin.at[t, most], send_sem=s_dis, recv_sem=r_dis, device_id=mate,
        device_id_type=MESH,
    )
    c_dis.wait()
    c_xf = send(xin.at[t], xin.at[t], s_xf, r_xf, mate)
    row, col = iota((256, 256), 0), iota((256, 256), 1)
    regroup = flag(
        (((row >> 6) == ((col >> 2) & 3)) & (((row >> 2) & 15) == (col >> 4))) & ((row & 3) == (col & 3))
    )
    ungroup = flag(
        (((col >> 6) == ((row >> 2) & 3)) & (((col >> 2) & 15) == (row >> 4))) & ((row & 3) == (col & 3))
    )
    c_xf.wait()
    for hf in range(2):
        for m in range(4):
            block = dot(regroup, xin[hf, m * 16 : (m + 1) * 16].reshape(256, 256)).astype(jnp.bfloat16)
            for q in range(4):
                xs[hf, m * 64 : (m + 1) * 64, q * 256 : (q + 1) * 256] = block[q * 64 : (q + 1) * 64]
    for w in wload:
        w.wait()
    g = dot(xs[0], wg[:HALF]) + dot(xs[1], wg[HALF:])
    u = dot(xs[0], wu[:HALF]) + dot(xs[1], wu[HALF:])
    act = (g / (1.0 + jnp.exp(-g)) * u).astype(jnp.bfloat16)
    for c in toks:
        c.wait()
    others = pl.ds(64, 448)
    c_fwd = send(tok.at[t, others, :], tok.at[t, others, :], s_fwd, r_fwd, mate)
    ybuf[0] = dot(act, wdn[:, :HALF])
    ybuf[1] = dot(act, wdn[:, HALF:])
    ysend[...] = ybuf[1 - t].astype(jnp.bfloat16)
    c_y = send(ysend, yrecv, s_y, r_y, mate)
    for c in legs:
        c.wait()
    c_fwd.wait()
    gate = dws[:, 0].reshape(384, 2048)
    up = dws[:, 1].reshape(384, 2048)
    down = dws[:, 2].reshape(384, 2048)

    def dense(p):
        part_rows = slice(p * 256, p * 256 + 256)
        t0, t1 = tok[0, part_rows, :], tok[1, part_rows, :]
        g = nt_dot(t0, gate[:, :HALF]) + nt_dot(t1, gate[:, HALF:])
        u = nt_dot(t0, up[:, :HALF]) + nt_dot(t1, up[:, HALF:])
        blend = 1.0 / (1.0 + jnp.exp(-g[:, 44:45]))
        act = (g / (1.0 + jnp.exp(-g)) * u).astype(jnp.bfloat16)
        dbuf[p, 0] = dot(act, down[:, :HALF]) * blend
        dbuf[p, 1] = dot(act, down[:, HALF:]) * blend
        dsend[p] = dbuf[p, 1 - t].astype(jnp.bfloat16)
        return send(dsend.at[p], drecv.at[p], s_dn.at[p], r_dn.at[p], mate)

    def homeward(p):
        rsend[p * 4 : p * 4 + 4] = (
            (dbuf[p, t] + drecv[p].astype(jnp.float32)).astype(jnp.bfloat16).reshape(4, 64, HALF)
        )

    c_dn = dense(0)
    c_y.wait()
    z = (ybuf[t] + yrecv[...].astype(jnp.float32)).astype(jnp.bfloat16)
    for m in range(4):
        block = jnp.concatenate([z[m * 64 : (m + 1) * 64, q * 256 : (q + 1) * 256] for q in range(4)], axis=0)
        zsend[m * 16 : (m + 1) * 16] = dot(ungroup, block).astype(jnp.bfloat16).reshape(16, 16, 256)

    def gather(k, _):
        e = (ep + k) % 64
        send(zsend.at[e], ret.at[ep], s_ret, r_ret, (e, t))
        return 0

    lax.fori_loop(1, 64, gather, 0)
    ret[ep] = zsend[ep]

    c_dn.wait()
    homeward(0)
    c_dn = dense(1)
    c_dn.wait()
    homeward(1)
    c_rs = []
    for m in range(3):
        cols, axis = pl.ds(*pieces[m]), order[m][0]
        for k in range(8):
            if k >> axis & 1:
                c_rs.append(send(
                    rsend.at[k, :, cols], rs.at[k - (1 << axis), :, cols], s_rs.at[m * 8 + k], r_rs.at[m * 8 + k],
                    b_peer(1 << axis),
                ))
    for c in c_rs:
        c.wait()
    c_rs, totals = [], []
    for m in range(3):
        cols, axis = slice(pieces[m][0], sum(pieces[m])), order[m][0]
        for k in range(8):
            if not k >> axis & 1:
                both = rsend[k, :, cols].astype(jnp.float32) + rs[k, :, cols].astype(jnp.float32)
                if k:
                    rsend[k, :, cols] = both.astype(jnp.bfloat16)
                    c_rs.append(send(
                        rsend.at[k, :, cols], rs2.at[k, :, cols], s_rs.at[m * 8 + k], r_rs.at[m * 8 + k], b_peer(k)
                    ))
                else:
                    totals.append(both)

    c_ret = pltpu.make_async_remote_copy(
        src_ref=zsend.at[most], dst_ref=ret.at[most], send_sem=s_ret, recv_sem=r_ret, device_id=mate,
        device_id_type=MESH,
    )
    c_ret.wait()
    comb = dot(pst[...], ret[...].reshape(1024, 256))
    for c in c_rs:
        c.wait()
    for m in range(3):
        cols, axis = slice(pieces[m][0], sum(pieces[m])), order[m][0]
        for k in range(1, 8):
            if not k >> axis & 1:
                totals[m] += rs2[k, :, cols].astype(jnp.float32)
    total = fres[t].astype(jnp.float32) + jnp.concatenate(totals, axis=1)
    for q in range(4):
        piece = slice(q * 256, (q + 1) * 256)
        obuf[t, :, piece] = (total[:, piece] + comb[q * 64 : (q + 1) * 64]).astype(jnp.bfloat16)
    c_out = send(obuf.at[t], obuf.at[t], s_out, r_out, mate)
    c_out.wait()
    stores[6].wait()
    stores[7].wait()
    out_ref[:, :HALF] = obuf[0]
    out_ref[:, HALF:] = obuf[1]


def layer(small, large):
    vm = pl.BlockSpec(memory_space=pltpu.VMEM)
    anyw = pl.BlockSpec(memory_space=pl.ANY)
    bf, f4 = jnp.bfloat16, jnp.float32
    dma = pltpu.SemaphoreType.DMA
    v = pltpu.VMEM
    scratch = [v((4, 8, 64, 64), f4), v((2, CH, 8, 64, 64), bf)] + [v(ref.shape, bf) for ref in large[:8]] + [
        v((2048, 512), bf), v((2048, 512), bf), v((2048, 512), bf), v((512, 2048), bf),
        v((4, CH, 8, 64, 64), f4),
        v((8, 64, 64), f4), v((8, 64, 64), f4), v((8, 64, 128), f4),
        v((64, 512), f4), v((2, 64, 2048), bf), v((2, 64, HALF), bf),
        v((2, 512, HALF), bf), v((2, 256, 256), bf), v((1024, 256), bf), v((256, 1024), bf),
        v((2048, 768), bf), v((2048, 768), bf), v((768, 2048), bf),
        v((8, 3, 48, 2048), bf),
        v((64, 16, 256), bf), v((2, 64, 16, 256), bf), v((2, 256, HALF), bf),
        v((2, 256, HALF), f4), v((256, HALF), bf), v((256, HALF), bf),
        v((64, 16, 256), bf), v((64, 16, 256), bf),
        v((2, 2, 256, HALF), f4), v((2, 256, HALF), bf), v((2, 256, HALF), bf),
        v((8, 64, HALF), bf), v((8, 64, HALF), bf), v((8, 64, HALF), bf), v((2, 64, HALF), bf),
        dma((8,)), dma((4,)), dma((8,)), dma((4,)), dma((8,)), dma((3,)), dma, dma, dma((24,)), dma((24,)), dma, dma, dma, dma, dma,
        dma, dma, dma, dma, dma, dma((2,)), dma((2,)), dma((24,)), dma((24,)), dma, dma, dma((24,)), dma((24,)),
    ]
    return pl.pallas_call(
        layer_kernel,
        out_shape=[jax.ShapeDtypeStruct((64, 2048), bf), jax.ShapeDtypeStruct((64, 8, 64, 64), bf)],
        in_specs=[vm] * len(small) + [anyw] * len(large),
        out_specs=[vm, anyw],
        scratch_shapes=scratch,
        compiler_params=pltpu.CompilerParams(
            collective_id=0, has_side_effects=True, vmem_limit_bytes=63 * 1024 * 1024
        ),
        name="layer",
    )(*small, *large)


SB = 4


def state_kernel(tokens_in, st_ref, ns_ref, out_ref, old, new, l_t, l_in, l_out):
    count = st_ref.shape[0] // SB

    def load(c):
        own = pl.ds(c * SB, SB)
        return pltpu.make_async_copy(st_ref.at[own], old.at[own], l_in.at[c])

    def store(c):
        own = pl.ds(c * SB, SB)
        return pltpu.make_async_copy(new.at[own], ns_ref.at[own], l_out.at[c])

    for c in range(count):
        load(c).start()
    tokens = pltpu.make_async_copy(tokens_in, out_ref, l_t)
    tokens.start()

    def one(c, _):
        load(c).wait()
        for u in range(SB):
            for h in range(8):
                new[c * SB + u, h] = old[c * SB + u, h].astype(jnp.float32)
        store(c).start()
        return 0

    lax.fori_loop(0, count, one, 0)
    tokens.wait()

    def drain(c, _):
        store(c).wait()
        return 0

    lax.fori_loop(0, count, drain, 0)


def wide_states(tokens, state):
    vm = pl.BlockSpec(memory_space=pltpu.VMEM)
    anyw = pl.BlockSpec(memory_space=pl.ANY)
    return pl.pallas_call(
        state_kernel,
        in_specs=[anyw, anyw],
        out_specs=[anyw, vm],
        out_shape=[
            jax.ShapeDtypeStruct(state.shape, jnp.float32),
            jax.ShapeDtypeStruct(tokens.shape, jnp.bfloat16),
        ],
        scratch_shapes=[
            pltpu.VMEM(state.shape, jnp.bfloat16),
            pltpu.VMEM(state.shape, jnp.float32),
            pltpu.SemaphoreType.DMA,
            pltpu.SemaphoreType.DMA((state.shape[0] // SB,)),
            pltpu.SemaphoreType.DMA((state.shape[0] // SB,)),
        ],
        compiler_params=pltpu.CompilerParams(vmem_limit_bytes=63 * 1024 * 1024),
        name="states",
    )(tokens, state)


def shards(
    hidden, mix_gain, recept_weight, key_weight, value_weight, decay_down, decay_up, decay_bias, rate_down, rate_up,
    rate_bias, head_gain, out_weight, memory_state, ffn_gain, blend_vector, dense_gate, dense_up, dense_down,
    expert_gate, expert_up, expert_down, routing, route_scale,
):
    flat = lambda vec: vec.reshape(1, -1)
    small = [
        flat(mix_gain), flat(decay_bias), flat(rate_bias), flat(head_gain), flat(ffn_gain), blend_vector.reshape(16, 128),
        routing.T, route_scale.T,
    ]
    large = [
        hidden, decay_down.T, decay_up, rate_down.T, rate_up, dense_gate.T, dense_up.T, dense_down,
        recept_weight, key_weight, value_weight, out_weight, memory_state, expert_gate, expert_up, expert_down,
    ]
    tokens, states = layer(small, large)
    new_state, layer_out = wide_states(tokens, states)
    return (layer_out, new_state)


def solution(mesh):
    in_specs = (
        P("ep", None),
        P(),
        P(None, "tp"),
        P(None, "tp"),
        P(None, "tp"),
        P(),
        P(),
        P(),
        P(),
        P(),
        P(),
        P(),
        P("tp", None),
        P("ep", "tp", None, None),
        P(),
        P(),
        P(None, ("ep", "tp")),
        P(None, ("ep", "tp")),
        P(("ep", "tp"), None),
        P("ep", None, "tp"),
        P("ep", None, "tp"),
        P("ep", "tp", None),
        P("ep", None),
        P("ep", None),
    )
    out_specs = (P("ep", None), P("ep", "tp", None, None))
    return jax.shard_map(shards, mesh=mesh, in_specs=in_specs, out_specs=out_specs, check_vma=False)
```

```python
import jax
import jax.numpy as jnp
from jax import lax
from jax.experimental import pallas as pl
from jax.experimental.pallas import tpu as pltpu
from jax.sharding import PartitionSpec as P

MESH = pl.DeviceIdType.MESH
CH = 8
HALF = 1024


def dot(a, b):
    return jnp.dot(a, b, preferred_element_type=jnp.float32)


def nt_dot(a, b):
    return lax.dot_general(a, b, (((1,), (1,)), ((), ())), preferred_element_type=jnp.float32)


def iota(shape, dim):
    return lax.broadcasted_iota(jnp.int32, shape, dim)


def flag(cond, dtype=jnp.bfloat16):
    return jnp.where(cond, 1.0, 0.0).astype(dtype)


def layer_kernel(
    mixg_ref, db_ref, rb_ref, hg_ref, fg_ref, bv_ref, route_ref, scale_ref,
    hid_in, dd_in, du_in, rd_in, ru_in, dg_in, dup_in, ddn_in, wr_ref, wk_ref, wv_ref, ow_ref, st_ref, eg_ref, eu_ref,
    ed_ref,
    out_ref, ns_ref,
    rows_ref, nsb, hid_ref, dd_ref, du_ref, rd_ref, ru_ref, dg_ref, dup_ref, ddn_ref, wr, wk, wv, ow, st, g_s, bt_s, yt_s, part, pbuf, fres, tok, tq, pbig, pst, wg, wu, wdn, dws, disp, xin, xs, ybuf,
    ysend, yrecv, zsend, ret, dbuf, dsend, drecv, rsend, rs, rs2, obuf,
    l_i, l_again, l_ns, l_a, l_s_sem, l_w, s_tp, r_tp, s_tok, r_tok, s_fwd, r_fwd, s_dis, r_dis, s_xf, r_xf, s_y, r_y, s_ret, r_ret,
    s_dn, r_dn, s_rs, r_rs, s_out, r_out, s_w, r_w,
):
    ep = lax.axis_index("ep")
    t = lax.axis_index("tp")
    place = (ep % 4, (ep // 4) % 4, ep // 16)
    mate = (ep, 1 - t)
    heads, size = 8, 64
    width = heads * size

    def chip(where):
        return (where[2] * 16 + where[1] * 4 + where[0], t)

    def b_peer(k):
        return chip([(c + 2 * ((k >> d) & 1)) % 4 for d, c in enumerate(place)])

    def beside(axis):
        step = [0, 0, 0]
        step[axis] = (1 - 2 * (place[axis] % 2)) * (1 - 2 * t) + 4
        return chip([(c + o) % 4 for c, o in zip(place, step)])

    k_s, d_s, l_s, v_s = rows_ref.at[0], rows_ref.at[1], rows_ref.at[2], rows_ref.at[3]
    iload = [
        pltpu.make_async_copy(src, dst, l_i.at[i])
        for i, (src, dst) in enumerate([
            (dg_in, dg_ref), (dup_in, dup_ref), (ddn_in, ddn_ref), (hid_in, hid_ref), (dd_in, dd_ref), (du_in, du_ref),
            (rd_in, rd_ref), (ru_in, ru_ref),
        ])
    ]
    for c in iload:
        c.start()
    barrier = pltpu.get_barrier_semaphore()
    pl.semaphore_signal(barrier, inc=1, device_id=mate, device_id_type=MESH)

    def greet(k, _):
        pl.semaphore_signal(barrier, inc=1, device_id=((ep + k) % 64, t), device_id_type=MESH)
        return 0

    lax.fori_loop(1, 64, greet, 0, unroll=7)

    aload = [
        pltpu.make_async_copy(src, dst, l_a.at[i])
        for i, (src, dst) in enumerate([(wk_ref, wk), (wr_ref, wr), (wv_ref, wv), (ow_ref, ow)])
    ]
    wload = [
        pltpu.make_async_copy(src.at[0], dst, l_w.at[i])
        for i, (src, dst) in enumerate([(eg_ref, wg), (eu_ref, wu), (ed_ref, wdn)])
    ]
    sload = [
        pltpu.make_async_copy(st_ref.at[pl.ds(c * CH, CH)], st.at[c % 4], l_s_sem.at[c]) for c in range(64 // CH)
    ]
    for c in aload[:3] + sload[:4] + aload[3:]:
        c.start()

    ids = iota((64, 64), 0).astype(jnp.float32)
    named = route_ref[...].astype(jnp.float32)
    one0, one1 = flag(named[0:1] == ids, jnp.float32), flag(named[1:2] == ids, jnp.float32)
    hit = one0 + one1
    scl = (one0 * scale_ref[0:1] + one1 * scale_ref[1:2]).astype(jnp.bfloat16)
    rank = dot(hit.astype(jnp.bfloat16), flag(iota((64, 64), 0) < iota((64, 64), 1)))
    rank = jnp.where(hit > 0.5, rank, -1.0).astype(jnp.bfloat16)
    tile = flag((iota((256, 64), 0) & 63) == iota((256, 64), 1))
    row, col = iota((1024, 256), 0), iota((1024, 256), 1)
    grown = dot(flag((iota((1024, 64), 0) >> 4) == iota((1024, 64), 1)), nt_dot(rank, tile).astype(jnp.bfloat16))
    pbig[...] = flag((grown == (row & 3).astype(jnp.float32)) & (((row >> 2) & 3) == (col >> 6)))
    row, col = iota((256, 1024), 0), iota((256, 1024), 1)
    spread = flag(iota((64, 1024), 0) == (iota((64, 1024), 1) >> 4))
    grown = dot(nt_dot(tile, rank).astype(jnp.bfloat16), spread)
    weight = dot(nt_dot(tile, scl).astype(jnp.bfloat16), spread)
    keep = (grown == (col & 3).astype(jnp.float32)) & (((col >> 2) & 3) == (row >> 6))
    pst[...] = jnp.where(keep, weight, 0.0).astype(jnp.bfloat16)

    for c in iload:
        c.wait()
    dws[0, :, 32:48, :] = jnp.zeros((3, 16, 2048), jnp.bfloat16)
    dws[0, 0, 0:44, :] = dg_ref[...]
    bv = bv_ref[...].astype(jnp.float32)
    dws[0, 0, 44:45, :] = jnp.concatenate([bv[i : i + 1] for i in range(16)], axis=1).astype(jnp.bfloat16)
    dws[0, 1, 0:44, :] = dup_ref[...]
    dws[0, 2, 0:44, :] = ddn_ref[...]

    def send(src, dst, s, r, dev):
        c = pltpu.make_async_remote_copy(
            src_ref=src, dst_ref=dst, send_sem=s, recv_sem=r, device_id=dev, device_id_type=MESH
        )
        c.start()
        return c

    pl.semaphore_wait(barrier, 64)

    def hop(m, held, axis):
        then = held + (1 << axis)
        sem = m * 8 + then
        return send(dws.at[held, m], dws.at[then, m], s_w.at[sem], r_w.at[sem], beside(axis))

    order = [[(m + i) % 3 for i in range(3)] for m in range(3)]
    legs = []
    leg_a = [hop(m, 0, order[m][0]) for m in range(3)]
    leg_b = [hop(m, 0, order[m][1]) for m in range(3)]
    legs += [hop(m, 0, order[m][2]) for m in range(3)]

    own = pl.ds(pl.multiple_of(t * width, width), width)
    xh = hid_ref[...].astype(jnp.float32)
    nb = (xh * lax.rsqrt(jnp.mean(xh * xh, axis=-1, keepdims=True) + 1e-06) * mixg_ref[...]).astype(jnp.bfloat16)
    low = jnp.tanh(nt_dot(nb, dd_ref[...])).astype(jnp.bfloat16)
    pre = dot(low, du_ref[:, own]) + db_ref[:, own]
    dec = jnp.exp(-jnp.exp(-0.5) * (1.0 / (1.0 + jnp.exp(-pre))))
    rlow = nt_dot(nb, rd_ref[...]).astype(jnp.bfloat16)
    lr = 1.0 / (1.0 + jnp.exp(-(dot(rlow, ru_ref[:, own]) + rb_ref[:, own])))
    for c in aload[:3]:
        c.wait()
    key = dot(nb, wk[...]).astype(jnp.bfloat16).astype(jnp.float32)
    rec = dot(nb, wr[...]).astype(jnp.bfloat16).astype(jnp.float32)
    val = dot(nb, wv[...]).astype(jnp.bfloat16).astype(jnp.float32)
    for h in range(heads):
        cut = slice(h * size, (h + 1) * size)
        kh, lh, rh, vh = key[:, cut], lr[:, cut], rec[:, cut], val[:, cut]
        kn = kh * (1.0 / (jnp.sum(kh * kh, axis=-1, keepdims=True) + 1e-06))
        kl = kh * lh
        beta = jnp.sum(kl * rh, axis=-1, keepdims=True)
        k_s[h] = kn
        d_s[h] = dec[:, cut]
        l_s[h] = kl
        v_s[h] = vh
        g_s[h] = dec[:, cut] * rh - beta * kn
        bt_s[h] = beta * vh

    for w in leg_a:
        w.wait()
    leg_c = [hop(m, 1 << order[m][0], order[m][1]) for m in range(3)]
    legs += [hop(m, 1 << order[m][0], order[m][2]) for m in range(3)]
    for w in leg_b:
        w.wait()
    legs += [hop(m, 1 << order[m][1], order[m][2]) for m in range(3)]

    lane = iota((size, 128), 1)
    chunks = 64 // CH
    for c in range(chunks):
        sload[c].wait()

        def one(j, _, c=c):
            for u in range(4):
                sl = j * 4 + u
                s = c * CH + sl
                for h in range(heads):
                    y = jnp.sum(st[c % 4, sl, h] * g_s[h, pl.ds(s, 1), :], axis=-1, keepdims=True)
                    yt_s[h] = jnp.where(lane == s, y, yt_s[h])
            return 0

        lax.fori_loop(0, CH // 4, one, 0)
        if c + 4 < chunks:
            sload[c + 4].start()
        if c == 3:
            for w in wload:
                w.start()
    eye = iota((size, size), 0) == iota((size, size), 1)
    again = [
        pltpu.make_async_copy(st_ref.at[pl.ds(c * CH, CH)], st.at[c % 4], l_again.at[c]) for c in range(4)
    ]
    stores = [
        pltpu.make_async_copy(nsb.at[n % 2], ns_ref.at[pl.ds((n + 4) % 8 * CH, CH)], l_ns.at[n]) for n in range(8)
    ]

    def update(n):
        c = (n + 4) % 8
        if n >= 4:
            again[c].wait()
        if n >= 2:
            stores[n - 2].wait()

        def one(j, _):
            for u in range(4):
                sl = j * 4 + u
                at = pl.ds(c * CH + sl, 1)
                for h in range(heads):
                    m = st[c % 4, sl, h]
                    w = jnp.sum(jnp.where(eye, v_s[h, at, :], 0.0) - m * k_s[h, at, :], axis=-1, keepdims=True)
                    nsb[n % 2, sl, h] = (m * d_s[h, at, :] + w * l_s[h, at, :]).astype(jnp.bfloat16)
            return 0

        lax.fori_loop(0, CH // 4, one, 0)
        stores[n].start()
        if n < 4:
            again[n].start()

    for h in range(heads):
        y = yt_s[h].T[:64] + bt_s[h]
        cen = y - jnp.mean(y, axis=-1, keepdims=True)
        var = jnp.mean(cen * cen, axis=-1, keepdims=True)
        part[:, h * size : (h + 1) * size] = cen * lax.rsqrt(var + 0.00064)
    hn = (part[:, :width] * hg_ref[:, own]).astype(jnp.bfloat16)
    aload[3].wait()
    pbuf[0] = dot(hn, ow[...]).astype(jnp.bfloat16)
    c_tp = send(pbuf.at[0], pbuf.at[1], s_tp, r_tp, mate)
    c_tp.wait()
    attn = pbuf[0].astype(jnp.float32) + pbuf[1].astype(jnp.float32)
    first = (hid_ref[...].astype(jnp.float32) + attn).astype(jnp.bfloat16)
    fres[0] = first[:, :HALF]
    fres[1] = first[:, HALF:]
    f32 = first.astype(jnp.float32)
    ffn = (
        f32 * lax.rsqrt(jnp.mean(f32 * f32, axis=-1, keepdims=True) + 1e-06) * fg_ref[...]
    ).astype(jnp.bfloat16)
    tok[0, 0:64, :] = ffn[:, :HALF]
    tok[1, 0:64, :] = ffn[:, HALF:]
    pieces = [(0, 384), (384, 384), (768, 256)]

    def pass_on(m, held, axis):
        then = held + (1 << axis)
        cols = pl.ds(*pieces[m])
        sem = m * 8 + then
        return send(
            tok.at[t, pl.ds(held * 64, 64), cols], tok.at[t, pl.ds(then * 64, 64), cols], s_tok.at[sem], r_tok.at[sem],
            b_peer(1 << axis),
        )

    tok_a = [pass_on(m, 0, order[m][0]) for m in range(3)]
    tok_b = [pass_on(m, 0, order[m][1]) for m in range(3)]
    toks = [pass_on(m, 0, order[m][2]) for m in range(3)]
    for q in range(8):
        tq[q // 4, (q % 4) * 64 : (q % 4 + 1) * 64, :] = ffn[:, q * 256 : (q + 1) * 256]
    disp[...] = dot(pbig[...], tq[t]).astype(jnp.bfloat16).reshape(64, 16, 256)

    def scatter(k, _):
        e = (ep + k) % 64
        send(disp.at[e], xin.at[t, ep], s_dis, r_dis, (e, t))
        return 0

    lax.fori_loop(1, 64, scatter, 0, unroll=7)
    xin[t, ep] = disp[ep]
    for n in range(3):
        update(n)
    for c in tok_a:
        c.wait()
    tok_c = [pass_on(m, 1 << order[m][0], order[m][1]) for m in range(3)]
    toks += [pass_on(m, 1 << order[m][0], order[m][2]) for m in range(3)]
    for c in tok_b:
        c.wait()
    toks += [pass_on(m, 1 << order[m][1], order[m][2]) for m in range(3)]
    for n in range(3, 6):
        update(n)
    for c in tok_c:
        c.wait()
    toks += [pass_on(m, (1 << order[m][0]) + (1 << order[m][1]), order[m][2]) for m in range(3)]
    for w in leg_c:
        w.wait()
    legs += [hop(m, (1 << order[m][0]) + (1 << order[m][1]), order[m][2]) for m in range(3)]
    for n in range(6, 8):
        update(n)
    most = pl.ds(0, 63)
    c_dis = pltpu.make_async_remote_copy(
        src_ref=disp.at[most], dst_ref=xin.at[t, most], send_sem=s_dis, recv_sem=r_dis, device_id=mate,
        device_id_type=MESH,
    )
    c_dis.wait()
    c_xf = send(xin.at[t], xin.at[t], s_xf, r_xf, mate)
    row, col = iota((256, 256), 0), iota((256, 256), 1)
    regroup = flag(
        (((row >> 6) == ((col >> 2) & 3)) & (((row >> 2) & 15) == (col >> 4))) & ((row & 3) == (col & 3))
    )
    ungroup = flag(
        (((col >> 6) == ((row >> 2) & 3)) & (((col >> 2) & 15) == (row >> 4))) & ((row & 3) == (col & 3))
    )
    c_xf.wait()
    for hf in range(2):
        for m in range(4):
            block = dot(regroup, xin[hf, m * 16 : (m + 1) * 16].reshape(256, 256)).astype(jnp.bfloat16)
            for q in range(4):
                xs[hf, m * 64 : (m + 1) * 64, q * 256 : (q + 1) * 256] = block[q * 64 : (q + 1) * 64]
    for w in wload:
        w.wait()
    g = dot(xs[0], wg[:HALF]) + dot(xs[1], wg[HALF:])
    u = dot(xs[0], wu[:HALF]) + dot(xs[1], wu[HALF:])
    act = (g / (1.0 + jnp.exp(-g)) * u).astype(jnp.bfloat16)
    for c in toks:
        c.wait()
    others = pl.ds(64, 448)
    c_fwd = send(tok.at[t, others, :], tok.at[t, others, :], s_fwd, r_fwd, mate)
    ybuf[0] = dot(act, wdn[:, :HALF])
    ybuf[1] = dot(act, wdn[:, HALF:])
    ysend[...] = ybuf[1 - t].astype(jnp.bfloat16)
    c_y = send(ysend, yrecv, s_y, r_y, mate)
    for c in legs:
        c.wait()
    c_fwd.wait()
    gate = dws[:, 0].reshape(384, 2048)
    up = dws[:, 1].reshape(384, 2048)
    down = dws[:, 2].reshape(384, 2048)

    def dense(p):
        part_rows = slice(p * 256, p * 256 + 256)
        t0, t1 = tok[0, part_rows, :], tok[1, part_rows, :]
        g = nt_dot(t0, gate[:, :HALF]) + nt_dot(t1, gate[:, HALF:])
        u = nt_dot(t0, up[:, :HALF]) + nt_dot(t1, up[:, HALF:])
        blend = 1.0 / (1.0 + jnp.exp(-g[:, 44:45]))
        act = (g / (1.0 + jnp.exp(-g)) * u).astype(jnp.bfloat16)
        dbuf[p, 0] = dot(act, down[:, :HALF]) * blend
        dbuf[p, 1] = dot(act, down[:, HALF:]) * blend
        dsend[p] = dbuf[p, 1 - t].astype(jnp.bfloat16)
        return send(dsend.at[p], drecv.at[p], s_dn.at[p], r_dn.at[p], mate)

    def homeward(p):
        rsend[p * 4 : p * 4 + 4] = (
            (dbuf[p, t] + drecv[p].astype(jnp.float32)).astype(jnp.bfloat16).reshape(4, 64, HALF)
        )

    c_dn = dense(0)
    c_y.wait()
    z = (ybuf[t] + yrecv[...].astype(jnp.float32)).astype(jnp.bfloat16)
    for m in range(4):
        block = jnp.concatenate([z[m * 64 : (m + 1) * 64, q * 256 : (q + 1) * 256] for q in range(4)], axis=0)
        zsend[m * 16 : (m + 1) * 16] = dot(ungroup, block).astype(jnp.bfloat16).reshape(16, 16, 256)

    def gather(k, _):
        e = (ep + k) % 64
        send(zsend.at[e], ret.at[ep], s_ret, r_ret, (e, t))
        return 0

    lax.fori_loop(1, 64, gather, 0, unroll=7)
    ret[ep] = zsend[ep]

    c_dn.wait()
    homeward(0)
    c_dn = dense(1)
    c_dn.wait()
    homeward(1)
    c_rs = []
    for m in range(3):
        cols, axis = pl.ds(*pieces[m]), order[m][0]
        for k in range(8):
            if k >> axis & 1:
                c_rs.append(send(
                    rsend.at[k, :, cols], rs.at[k - (1 << axis), :, cols], s_rs.at[m * 8 + k], r_rs.at[m * 8 + k],
                    b_peer(1 << axis),
                ))
    for c in c_rs:
        c.wait()
    c_rs, totals = [], []
    for m in range(3):
        cols, axis = slice(pieces[m][0], sum(pieces[m])), order[m][0]
        for k in range(8):
            if not k >> axis & 1:
                both = rsend[k, :, cols].astype(jnp.float32) + rs[k, :, cols].astype(jnp.float32)
                if k:
                    rsend[k, :, cols] = both.astype(jnp.bfloat16)
                    c_rs.append(send(
                        rsend.at[k, :, cols], rs2.at[k, :, cols], s_rs.at[m * 8 + k], r_rs.at[m * 8 + k], b_peer(k)
                    ))
                else:
                    totals.append(both)

    c_ret = pltpu.make_async_remote_copy(
        src_ref=zsend.at[most], dst_ref=ret.at[most], send_sem=s_ret, recv_sem=r_ret, device_id=mate,
        device_id_type=MESH,
    )
    c_ret.wait()
    comb = dot(pst[...], ret[...].reshape(1024, 256))
    for c in c_rs:
        c.wait()
    for m in range(3):
        cols, axis = slice(pieces[m][0], sum(pieces[m])), order[m][0]
        for k in range(1, 8):
            if not k >> axis & 1:
                totals[m] += rs2[k, :, cols].astype(jnp.float32)
    total = fres[t].astype(jnp.float32) + jnp.concatenate(totals, axis=1)
    for q in range(4):
        piece = slice(q * 256, (q + 1) * 256)
        obuf[t, :, piece] = (total[:, piece] + comb[q * 64 : (q + 1) * 64]).astype(jnp.bfloat16)
    c_out = send(obuf.at[t], obuf.at[t], s_out, r_out, mate)
    c_out.wait()
    stores[6].wait()
    stores[7].wait()
    out_ref[:, :HALF] = obuf[0]
    out_ref[:, HALF:] = obuf[1]


def layer(small, large):
    vm = pl.BlockSpec(memory_space=pltpu.VMEM)
    anyw = pl.BlockSpec(memory_space=pl.ANY)
    bf, f4 = jnp.bfloat16, jnp.float32
    dma = pltpu.SemaphoreType.DMA
    v = pltpu.VMEM
    scratch = [v((4, 8, 64, 64), f4), v((2, CH, 8, 64, 64), bf)] + [v(ref.shape, bf) for ref in large[:8]] + [
        v((2048, 512), bf), v((2048, 512), bf), v((2048, 512), bf), v((512, 2048), bf),
        v((4, CH, 8, 64, 64), f4),
        v((8, 64, 64), f4), v((8, 64, 64), f4), v((8, 64, 128), f4),
        v((64, 512), f4), v((2, 64, 2048), bf), v((2, 64, HALF), bf),
        v((2, 512, HALF), bf), v((2, 256, 256), bf), v((1024, 256), bf), v((256, 1024), bf),
        v((2048, 768), bf), v((2048, 768), bf), v((768, 2048), bf),
        v((8, 3, 48, 2048), bf),
        v((64, 16, 256), bf), v((2, 64, 16, 256), bf), v((2, 256, HALF), bf),
        v((2, 256, HALF), f4), v((256, HALF), bf), v((256, HALF), bf),
        v((64, 16, 256), bf), v((64, 16, 256), bf),
        v((2, 2, 256, HALF), f4), v((2, 256, HALF), bf), v((2, 256, HALF), bf),
        v((8, 64, HALF), bf), v((8, 64, HALF), bf), v((8, 64, HALF), bf), v((2, 64, HALF), bf),
        dma((8,)), dma((4,)), dma((8,)), dma((4,)), dma((8,)), dma((3,)), dma, dma, dma((24,)), dma((24,)), dma, dma, dma, dma, dma,
        dma, dma, dma, dma, dma, dma((2,)), dma((2,)), dma((24,)), dma((24,)), dma, dma, dma((24,)), dma((24,)),
    ]
    return pl.pallas_call(
        layer_kernel,
        out_shape=[jax.ShapeDtypeStruct((64, 2048), bf), jax.ShapeDtypeStruct((64, 8, 64, 64), bf)],
        in_specs=[vm] * len(small) + [anyw] * len(large),
        out_specs=[vm, anyw],
        scratch_shapes=scratch,
        compiler_params=pltpu.CompilerParams(
            collective_id=0, has_side_effects=True, vmem_limit_bytes=63 * 1024 * 1024
        ),
        name="layer",
    )(*small, *large)


SB = 4


def state_kernel(tokens_in, st_ref, ns_ref, out_ref, old, new, l_t, l_in, l_out):
    count = st_ref.shape[0] // SB

    def load(c):
        own = pl.ds(c * SB, SB)
        return pltpu.make_async_copy(st_ref.at[own], old.at[own], l_in.at[c])

    def store(c):
        own = pl.ds(c * SB, SB)
        return pltpu.make_async_copy(new.at[own], ns_ref.at[own], l_out.at[c])

    for c in range(count):
        load(c).start()
    tokens = pltpu.make_async_copy(tokens_in, out_ref, l_t)
    tokens.start()

    def one(c, _):
        load(c).wait()
        for u in range(SB):
            for h in range(8):
                new[c * SB + u, h] = old[c * SB + u, h].astype(jnp.float32)
        store(c).start()
        return 0

    lax.fori_loop(0, count, one, 0)
    tokens.wait()

    def drain(c, _):
        store(c).wait()
        return 0

    lax.fori_loop(0, count, drain, 0)


def wide_states(tokens, state):
    vm = pl.BlockSpec(memory_space=pltpu.VMEM)
    anyw = pl.BlockSpec(memory_space=pl.ANY)
    return pl.pallas_call(
        state_kernel,
        in_specs=[anyw, anyw],
        out_specs=[anyw, vm],
        out_shape=[
            jax.ShapeDtypeStruct(state.shape, jnp.float32),
            jax.ShapeDtypeStruct(tokens.shape, jnp.bfloat16),
        ],
        scratch_shapes=[
            pltpu.VMEM(state.shape, jnp.bfloat16),
            pltpu.VMEM(state.shape, jnp.float32),
            pltpu.SemaphoreType.DMA,
            pltpu.SemaphoreType.DMA((state.shape[0] // SB,)),
            pltpu.SemaphoreType.DMA((state.shape[0] // SB,)),
        ],
        compiler_params=pltpu.CompilerParams(vmem_limit_bytes=63 * 1024 * 1024),
        name="states",
    )(tokens, state)


def shards(
    hidden, mix_gain, recept_weight, key_weight, value_weight, decay_down, decay_up, decay_bias, rate_down, rate_up,
    rate_bias, head_gain, out_weight, memory_state, ffn_gain, blend_vector, dense_gate, dense_up, dense_down,
    expert_gate, expert_up, expert_down, routing, route_scale,
):
    flat = lambda vec: vec.reshape(1, -1)
    small = [
        flat(mix_gain), flat(decay_bias), flat(rate_bias), flat(head_gain), flat(ffn_gain), blend_vector.reshape(16, 128),
        routing.T, route_scale.T,
    ]
    large = [
        hidden, decay_down.T, decay_up, rate_down.T, rate_up, dense_gate.T, dense_up.T, dense_down,
        recept_weight, key_weight, value_weight, out_weight, memory_state, expert_gate, expert_up, expert_down,
    ]
    tokens, states = layer(small, large)
    new_state, layer_out = wide_states(tokens, states)
    return (layer_out, new_state)


def solution(mesh):
    in_specs = (
        P("ep", None),
        P(),
        P(None, "tp"),
        P(None, "tp"),
        P(None, "tp"),
        P(),
        P(),
        P(),
        P(),
        P(),
        P(),
        P(),
        P("tp", None),
        P("ep", "tp", None, None),
        P(),
        P(),
        P(None, ("ep", "tp")),
        P(None, ("ep", "tp")),
        P(("ep", "tp"), None),
        P("ep", None, "tp"),
        P("ep", None, "tp"),
        P("ep", "tp", None),
        P("ep", None),
        P("ep", None),
    )
    out_specs = (P("ep", None), P("ep", "tp", None, None))
    return jax.shard_map(shards, mesh=mesh, in_specs=in_specs, out_specs=out_specs, check_vma=False)
```
